32 devices in a mesh: gr: 2 (over x), fs: 8 (over z, y), tp: 2 (over core).
Axes of the slice: x: 2, y: 2, z: 4, core: 2. Of those that a mesh axis runs over, the one named last changes fastest.
Arguments:
- prompt: bfloat16 [4, 256, 2048], P(('gr', 'tp')), as said below
- norm_gain: float32 [2, 2048], P(None, 'fs'), may hold values from 0.1 to 1.9
- gate_weight: float32 [2, 2048, 4096], P(None, 'fs', ('gr', 'tp')), may hold values from -0.125 to 0.125
- up_weight: float32 [2, 2048, 4096], P(None, 'fs', ('gr', 'tp')), may hold values from -0.125 to 0.125
- down_weight: float32 [2, 4096, 2048], P(None, 'fs', ('gr', 'tp')), may hold values from -0.09375 to 0.09375
Outputs:
- gate_sampler: bfloat16 [2, 2048, 4096], P(None, None, 'fs')
- up_sampler: bfloat16 [2, 2048, 4096], P(None, None, 'fs')
- down_sampler: bfloat16 [2, 4096, 2048], P(None, 'fs')
- mixed: bfloat16 [4, 256, 2048], P(('gr', 'tp'))
The draws below stay inside these ranges and needn't reach their ends.
Inputs may be any that keep to these rules, and one draw needn't show every extreme that they name: prompt features have scales that differ from feature to feature.
All inputs are finite; a program needn't handle non-finite values.
Results may differ from the reference program's by a relative error of at most 0.0043.
Values may be sent and summed in bfloat16 or wider, within the bound.
A program may use at most 64 MiB of HBM per device.

```python
import jax
import jax.numpy as jnp
from jax import lax

D = 2048
FF = 4096
ROWS = 256
REQS = 4


def draw_prompt(key, part):
    first = jax.random.fold_in(jax.random.fold_in(key, 7), 0)
    column = jnp.arange(D, dtype=jnp.float32) / (D - 1.0)
    values = jax.random.normal(first, (REQS, ROWS, D), jnp.float32)
    scales = jnp.exp(column * 1.1)
    values = values * scales[None, None, :] * 0.6
    return jnp.clip(values, -6.0, 6.0).astype(jnp.bfloat16)


def level_of(key, extent, pieces, smallest, high):
    loudness, own = 1.0, jax.random.fold_in(key, 6)
    for dim, shards_of in pieces:
        steps = jnp.exp(jax.random.uniform(jax.random.fold_in(own, dim), (shards_of,), jnp.float32, smallest / len(pieces), high / len(pieces)))
        loudness = loudness * jnp.repeat(steps, extent[dim] // shards_of).reshape([-1 if axis == dim else 1 for axis in range(len(extent))])
    return loudness


def centred(rng, extent, scale, most, pieces=(), held_as=jnp.bfloat16):
    entries = jax.random.normal(rng, extent, jnp.float32) * scale
    if len(pieces) > 0:
        entries = level_of(rng, extent, pieces, -0.22, 0.18) * entries
    return jnp.clip(entries, min=-most, max=most).astype(held_as)


def setup_inputs(seed: int = 0) -> dict:
    splits = jax.random.split(jax.random.key(seed), 6)
    prompt = draw_prompt(jax.random.fold_in(splits[5], 71), 0)
    norm_gain = jnp.clip(1.0 + 0.18 * jax.random.normal(splits[1], (2, D), jnp.float32), 0.1, 1.9)
    gate_weight = centred(splits[2], (2, D, FF), D ** -0.5, 0.125, ((1, 8), (2, 4)), jnp.float32)
    up_weight = centred(splits[3], (2, D, FF), D ** -0.5, 0.125, ((1, 8), (2, 4)), jnp.float32)
    down_weight = centred(splits[4], (2, FF, D), FF ** -0.5, 0.09375, ((1, 8), (2, 4)), jnp.float32)
    return {"prompt": prompt, "norm_gain": norm_gain, "gate_weight": gate_weight, "up_weight": up_weight, "down_weight": down_weight}


norm_eps = 1e-06

def reference(prompt, norm_gain, gate_weight, up_weight, down_weight):
    gates = (norm_gain[:, :, None] * gate_weight).astype(jnp.bfloat16)
    ups = (norm_gain[:, :, None] * up_weight).astype(jnp.bfloat16)
    downs = down_weight.astype(jnp.bfloat16)
    total_rows = prompt.shape[0] * prompt.shape[1]
    stream = prompt.astype(jnp.float32).reshape(total_rows, D)
    for half_step in range(2):
        normed = (stream * lax.rsqrt(lax.optimization_barrier(jnp.mean(stream * stream, axis=-1, keepdims=True)) + norm_eps)).astype(jnp.bfloat16)
        gate_act = jnp.dot(normed, gates[half_step], preferred_element_type=jnp.float32)
        up_act = jnp.dot(normed, ups[half_step], preferred_element_type=jnp.float32)
        hidden = (jax.nn.silu(gate_act) * up_act).astype(jnp.bfloat16)
        projected = jnp.dot(hidden, downs[half_step], preferred_element_type=jnp.float32)
        stream = stream + 0.5 * projected
    mixed = stream.astype(jnp.bfloat16).reshape(prompt.shape)
    return (gates, ups, downs, mixed)
```

```python
import functools

import jax
import jax.numpy as jnp
from jax import lax
from jax.experimental import pallas as pl
from jax.experimental.pallas import tpu as pltpu
from jax.sharding import PartitionSpec as P

norm_eps = 1e-06
MESH = pl.DeviceIdType.MESH
f32 = jnp.float32
bf16 = jnp.bfloat16


def kernel(G, n, T, prompt, gain, gate_w, up_w, down_w,
           wall, dn, ag,
           wsrc, p, r1, q2, r2, lhs, hid, st,
           x_s, x_r, v_s, v_r, xd_s, p_s, w_r, w_l, f_s, d_s, d_r,
           s1_s, s1_r, s2_s, s2_r, g_s, gg_s, g_r, h_s):
    gr, fs, tp = lax.axis_index("gr"), lax.axis_index("fs"), lax.axis_index("tp")
    q, R, FFb = wsrc.shape[3:]
    tb, D = prompt.shape[1:]
    rows = n * tb
    DC = dn.shape[3]
    na = n // 2
    a, b = fs // 2, lax.rem(fs, 2)
    C = s1_s.shape[2]
    tc = tb // C
    peer = fs + 1 - 2 * b
    is_recv = lax.rem(fs // q, T) == tp
    slot_me = gr * T + tp
    hs = [(R * c // 16) // 16 * 16 if G == 2 else 0 for c in (4, 8)]

    def mine(k, g):
        return pl.ds(pl.multiple_of(g * hs[k], 16), R - hs[k]) if hs[k] else pl.ds(0, R)

    def only(k, g):
        return pl.ds(pl.multiple_of(g * (R - hs[k]), 16), hs[k])

    def dev(g, f, t):
        return {"gr": g, "fs": f, "tp": t}

    def rc(src, dst, ss, rs, d):
        return pltpu.make_async_remote_copy(
            src_ref=src, dst_ref=dst, send_sem=ss, recv_sem=rs,
            device_id=d, device_id_type=MESH)

    def loop(lo, hi, body):
        def step(i, c):
            body(i)
            return c
        lax.fori_loop(lo, hi, step, 0)

    others_g = [lax.rem(gr + d, G) for d in range(1, G)]
    others_t = [lax.rem(tp + d, T) for d in range(1, T)]

    def x_copy(k, w, i, g_src, g_dst):
        blk = wsrc.at[k, w, g_src, i, mine(k, g_dst)]
        return rc(blk, blk, x_s.at[k, w, i, g_dst], x_r.at[k, w, i, g_src], dev(g_dst, fs, tp))

    def xd_copy(k, g_src, g_dst):
        blk = dn.at[k, g_src * T + tp]
        return rc(blk, blk, xd_s.at[k, g_dst], d_r.at[k, g_src * T + tp], dev(g_dst, fs, tp))

    def d_copy(k, g_src, t_src, t_dst):
        blk = dn.at[k, g_src * T + t_src]
        return rc(blk, blk, d_s.at[k, g_src, t_dst], d_r.at[k, g_src * T + t_src], dev(gr, fs, t_dst))

    def col_of(g, i):
        return (g * T + tp) * q + i

    def p_copy(k, w, g, i):
        return rc(wsrc.at[k, w, g, i, mine(k, gr)], wall.at[k, w, fs, mine(k, gr)], p_s.at[k, w, g, i],
                  w_r.at[k, w, fs], dev(gr, col_of(g, i), tp))

    def l_copy(k, w, g, i):
        return pltpu.make_async_copy(wsrc.at[k, w, g, i, mine(k, gr)], wall.at[k, w, fs, mine(k, gr)], w_l.at[k, w])

    def f_copy(k, w, f, t):
        blk = wall.at[k, w, f, mine(k, gr)]
        return rc(blk, blk, f_s.at[k, w, 0, f, t], w_r.at[k, w, f], dev(gr, fs, t))

    def v_copy(k, w, f, g_src):
        blk = wall.at[k, w, f, only(k, g_src)]
        return rc(blk, blk, v_s.at[k, w, f], v_r.at[k, w, 0, f], dev(1 - g_src, fs, tp))

    def fv_copy(k, w, f, t):
        blk = wall.at[k, w, f, only(k, 1 - gr)]
        return rc(blk, blk, f_s.at[k, w, 1, f, t], v_r.at[k, w, 1, f], dev(gr, fs, t))

    def cast_w(k, w):
        ref = (gate_w, up_w)[w]
        for i in range(q):
            wsrc[k, w, gr, i] = (gain[k] * ref[k, :, i * FFb:(i + 1) * FFb]).astype(bf16)

    def xsend_w(k, w):
        for i in range(q):
            for g in others_g:
                x_copy(k, w, i, gr, g).start()

    def cast_d(k):
        dn[k, slot_me] = down_w[k].astype(bf16)

    def xsend_d(k):
        for g in others_g:
            xd_copy(k, gr, g).start()
        for t in others_t:
            d_copy(k, gr, tp, t).start()

    def plane(k, w, g, i):
        c = col_of(g, i)

        @pl.when(c != fs)
        def _():
            p_copy(k, w, g, i).start()

        @pl.when(c == fs)
        def _():
            l_copy(k, w, g, i).start()

    def plane_own(k, w):
        for i in range(q):
            plane(k, w, gr, i)

    def plane_x(k, w):
        for g in others_g:
            for i in range(q):
                x_copy(k, w, i, g, gr).wait_recv()
                plane(k, w, g, i)

    def arrive(k, w):
        def forward(f):
            for t in others_t:
                f_copy(k, w, f, t).start()
            if hs[k]:
                v_copy(k, w, f, gr).start()

        @pl.when(is_recv)
        def _():
            l_copy(k, w, 0, 0).wait()
            forward(fs)

            def take(s):
                f = lax.rem(fs + s, n)
                f_copy(k, w, f, tp).wait_recv()
                forward(f)
            loop(1, n, take)

    def cross(k, w):
        if hs[k]:
            @pl.when(is_recv)
            def _():
                def take(s):
                    f = lax.rem(fs + s, n)
                    v_copy(k, w, f, 1 - gr).wait_recv()
                    for t in others_t:
                        fv_copy(k, w, f, t).start()
                loop(0, n, take)

    def landed(k, w):
        @pl.when(jnp.logical_not(is_recv))
        def _():
            def take(f):
                f_copy(k, w, f, tp).wait_recv()
                if hs[k]:
                    fv_copy(k, w, f, tp).wait_recv()
            loop(0, n, take)

    def relay_d(k):
        for g in others_g:
            xd_copy(k, g, gr).wait_recv()
            for t in others_t:
                d_copy(k, g, tp, t).start()

    def landed_d(k):
        for g in range(G):
            for t in others_t:
                d_copy(k, g, t, tp).wait_recv()

    def gather_done(k):
        for w in range(2):
            for i in range(q):
                for g in others_g:
                    x_copy(k, w, i, gr, g).wait_send()
            for g in range(G):
                for i in range(q):
                    @pl.when(col_of(g, i) != fs)
                    def _():
                        p_copy(k, w, g, i).wait_send()

            @pl.when(is_recv)
            def _():
                def sent(f):
                    for t in others_t:
                        f_copy(k, w, f, t).wait_send()
                        if hs[k]:
                            fv_copy(k, w, f, t).wait_send()
                    if hs[k]:
                        v_copy(k, w, f, gr).wait_send()
                loop(0, n, sent)
        for g in others_g:
            xd_copy(k, gr, g).wait_send()
        for g in range(G):
            for t in others_t:
                d_copy(k, g, tp, t).wait_send()

    def flatten(ref):
        cw = 256

        def chunk(j):
            cols = pl.ds(pl.multiple_of(j * cw, cw), cw)
            lhs[:, cols] = ref[:, :, cols].astype(f32).reshape(rows, cw).astype(bf16)
        loop(0, D // cw, chunk)

    def normed_of(x):
        return (x * lax.rsqrt(jnp.mean(x * x, axis=-1, keepdims=True) + norm_eps)).astype(bf16)

    def compute(k):
        ft = min(FFb, 256)

        def act(j):
            cols = pl.ds(pl.multiple_of(j * ft, ft), ft)
            gate = jnp.dot(lhs[...], wall[k, 0, :, :, cols].reshape(D, ft), preferred_element_type=f32)
            up = jnp.dot(lhs[...], wall[k, 1, :, :, cols].reshape(D, ft), preferred_element_type=f32)
            hid[:, cols] = (gate / (1.0 + jnp.exp(-gate)) * up).astype(bf16)
        loop(0, FFb // ft, act)

        def proj(s):
            cols = pl.ds(pl.multiple_of(s * DC, DC), DC)
            v = jnp.dot(hid[...], dn[k, s], preferred_element_type=f32)
            p[k, :, :, cols] = v.reshape(n, tb, DC).astype(bf16)
        loop(0, G * T, proj)

    half = na // 2 if na % 2 == 0 else na
    far = na // half - 1
    pos = lax.rem(a, half)
    mirror = lax.rem(a + half, na)

    def near(d):
        return a - pos + lax.rem(pos + d, half)

    def partner(d):
        e = lax.div(d, half) if far else 1
        return lax.rem(a // half + 1 - e, far + 1) * half + lax.rem(pos + d + (e if far else 1), half)

    def part(c):
        return pl.ds(c * tc, tc)

    def s1_copy(k, a2, c):
        return rc(p.at[k, 2 * a2 + 1 - b, part(c)], r1.at[k, a2, part(c)],
                  s1_s.at[k, a2, c], s1_r.at[k, a2, c], dev(gr, peer, tp))

    def s2_copy(k, a2, a_from, c):
        return rc(q2.at[k, a2, part(c)], r2.at[k, a_from, part(c)],
                  s2_s.at[k, a2, c], s2_r.at[k, a_from, c], dev(gr, 2 * a2 + b, tp))

    def rs_first(k):
        for c in range(C):
            def send(d):
                s1_copy(k, partner(d), c).start()
            loop(0, na - 1, send)
            s1_copy(k, a, c).start()

    def rs_remote(k, c):
        def send(d):
            a2 = partner(d)
            s1_copy(k, a2, c).wait_recv()
            q2[k, a2, part(c)] = (p[k, 2 * a2 + b, part(c)].astype(f32) + r1[k, a2, part(c)].astype(f32)).astype(bf16)
            s2_copy(k, a2, a, c).start()
        loop(0, na - 1, send)

    def rs_own(k, c):
        s1_copy(k, a, c).wait_recv()
        st[part(c)] += 0.5 * (p[k, fs, part(c)].astype(f32) + r1[k, a, part(c)].astype(f32))

    def rs_last(k, c):
        def take(d):
            a2 = partner(na - 2 - d)
            s2_copy(k, a2, a2, c).wait_recv()
            st[part(c)] += 0.5 * r2[k, a2, part(c)].astype(f32)
        loop(0, na - 1, take)
        x = st[part(c)]
        ag[k, fs, part(c)] = normed_of(x) if k == 0 else x.astype(bf16)

        if far:
            z_copy(k, fs, mirror, c).start()

        def send(d):
            z_copy(k, fs, near(d), c).start()
        loop(1, half, send)
        y_copy(k, fs, c).start()

    def z_copy(k, j, a2, c):
        blk = ag.at[k, j, part(c)]
        return rc(blk, blk, g_s.at[k, a2, c], g_r.at[k, j, c], dev(gr, 2 * a2 + b, tp))

    def y_copy(k, j, c):
        blk = ag.at[k, j, part(c)]
        return rc(blk, blk, h_s.at[k, j // 2, c], g_r.at[k, j, c], dev(gr, peer, tp))

    def zz_copy(k, a2, c):
        blk = ag.at[k, 2 * mirror + b, part(c)]
        return rc(blk, blk, gg_s.at[k, a2, c], g_r.at[k, 2 * mirror + b, c], dev(gr, 2 * a2 + b, tp))

    def ag_relay(k, c):
        def pass_on(a2):
            z_copy(k, 2 * a2 + b, a2, c).wait_recv()
            y_copy(k, 2 * a2 + b, c).start()

        def own(d):
            pass_on(near(d))
        loop(1, half, own)
        if far:
            z_copy(k, 2 * mirror + b, a, c).wait_recv()

            def spread(d):
                zz_copy(k, near(d), c).start()
            loop(1, half, spread)
            y_copy(k, 2 * mirror + b, c).start()

            def theirs(d):
                pass_on(lax.rem(near(d) + half, na))
            loop(1, half, theirs)

    def ag_take(k):
        for c in range(C):
            def take(a2):
                y_copy(k, 2 * a2 + 1 - b, c).wait_recv()
            loop(0, na, take)

    def rs_done(k):
        for c in range(C):
            def sent(a2):
                s1_copy(k, a2, c).wait_send()
            loop(0, na, sent)

            def sent2(d):
                s2_copy(k, partner(d), a, c).wait_send()
            loop(0, na - 1, sent2)

    def ag_done(k):
        for c in range(C):
            def sent(d):
                z_copy(k, fs, near(d), c).wait_send()
                if far:
                    zz_copy(k, near(d), c).wait_send()
            loop(1, half, sent)
            if far:
                z_copy(k, fs, mirror, c).wait_send()

            def sent2(a2):
                y_copy(k, 2 * a2 + b, c).wait_send()
            loop(0, na, sent2)

    barrier = pltpu.get_barrier_semaphore()

    def greet(s):
        pl.semaphore_signal(barrier, inc=1, device_id=dev(gr, lax.rem(fs + s, n), tp), device_id_type=MESH)
    loop(1, n, greet)
    for t in others_t:
        pl.semaphore_signal(barrier, inc=1, device_id=dev(gr, fs, t), device_id_type=MESH)
    for g in others_g:
        pl.semaphore_signal(barrier, inc=1, device_id=dev(g, fs, tp), device_id_type=MESH)
    cast_w(0, 0)
    pl.semaphore_wait(barrier, n + T + G - 3)

    def norm_rows(j):
        p[0, j] = normed_of(prompt[j].astype(f32))

    def start_tokens():
        loop(0, n, norm_rows)
        flatten(p.at[0])
        st[...] = prompt[fs].astype(f32)

    def unpack(k):
        flatten(ag.at[k])

    def done(k):
        gather_done(k)
        rs_done(k)
        ag_done(k)

    xsend_w(0, 0)
    plane_own(0, 0)
    cast_w(0, 1)
    xsend_w(0, 1)
    plane_own(0, 1)
    cast_d(0)
    xsend_d(0)
    cast_w(1, 0)
    cast_w(1, 1)
    cast_d(1)
    start_tokens()
    xsend_w(1, 0)
    plane_x(0, 0)
    plane_x(0, 1)
    plane_own(1, 0)
    arrive(0, 0)
    xsend_w(1, 1)
    plane_x(1, 0)
    plane_own(1, 1)
    arrive(0, 1)
    relay_d(0)
    cross(0, 0)
    cross(0, 1)
    landed(0, 0)
    landed(0, 1)
    plane_x(1, 1)
    xsend_d(1)
    landed_d(0)
    compute(0)
    rs_first(0)
    arrive(1, 0)
    rs_remote(0, 0)
    rs_own(0, 0)
    if C > 1:
        rs_remote(0, 1)
    if C > 1:
        rs_last(0, 0)
    if C > 1:
        rs_own(0, 1)
    arrive(1, 1)
    rs_last(0, C - 1)
    relay_d(1)
    ag_relay(0, 0)
    cross(1, 0)
    if C > 1:
        ag_relay(0, 1)
    ag_take(0)
    unpack(0)
    cross(1, 1)
    landed(1, 0)
    landed(1, 1)
    landed_d(1)
    compute(1)
    rs_first(1)
    rs_remote(1, 0)
    rs_own(1, 0)
    if C > 1:
        rs_remote(1, 1)
    if C > 1:
        rs_last(1, 0)
    if C > 1:
        rs_own(1, 1)
    rs_last(1, C - 1)
    ag_relay(1, 0)
    if C > 1:
        ag_relay(1, 1)
    ag_take(1)
    done(0)
    done(1)

def write_out(wall, dn, ag, gate_o, up_o, down_o, mixed_o, o_s, d_s, m_s):
    L, S, _, DC = dn.shape
    copies = []
    for k in range(L):
        copies.append(pltpu.make_async_copy(wall.at[k, 0], gate_o.at[k], o_s.at[k, 0]))
        copies.append(pltpu.make_async_copy(wall.at[k, 1], up_o.at[k], o_s.at[k, 1]))
        for s in range(S):
            copies.append(pltpu.make_async_copy(
                dn.at[k, s], down_o.at[k, :, pl.ds(s * DC, DC)], d_s.at[k, s]))
    copies.append(pltpu.make_async_copy(ag.at[L - 1], mixed_o, m_s))
    for c in copies:
        c.start()
    for c in copies:
        c.wait()


def per_device(G, n, T, prompt, norm_gain, gate_weight, up_weight, down_weight):
    D = prompt.shape[2]
    rows = prompt.shape[0] * prompt.shape[1]
    L, R, C = gate_weight.shape
    FFb, DC = down_weight.shape[1:]
    q = C // FFb
    tb = rows // n
    na = n // 2
    C = max(1, min(2, tb // 8))
    dma = pltpu.SemaphoreType.DMA
    vmem = pl.BlockSpec(memory_space=pltpu.VMEM)
    anym = pl.BlockSpec(memory_space=pl.ANY)
    wall, dn, ag = pl.pallas_call(
        functools.partial(kernel, G, n, T),
        out_shape=(
            pltpu.VMEM((L, 2, n, R, FFb), bf16),
            pltpu.VMEM((L, G * T, FFb, DC), bf16),
            pltpu.VMEM((L, n, tb, D), bf16),
        ),
        in_specs=[vmem] * 5,
        out_specs=(vmem,) * 3,
        scratch_shapes=[
            pltpu.VMEM((L, 2, G, q, R, FFb), bf16),
            pltpu.VMEM((L, n, tb, D), bf16),
            pltpu.VMEM((L, na, tb, D), bf16),
            pltpu.VMEM((L, na, tb, D), bf16),
            pltpu.VMEM((L, na, tb, D), bf16),
            pltpu.VMEM((rows, D), bf16),
            pltpu.VMEM((rows, FFb), bf16),
            pltpu.VMEM((tb, D), f32),
            dma((L, 2, q, G)), dma((L, 2, q, G)), dma((L, 2, n)), dma((L, 2, 2, n)), dma((L, G)),
            dma((L, 2, G, q)), dma((L, 2, n)), dma((L, 2)), dma((L, 2, 2, n, T)),
            dma((L, G, T)), dma((L, G * T)),
            dma((L, na, C)), dma((L, na, C)), dma((L, na, C)), dma((L, na, C)),
            dma((L, na, C)), dma((L, na, C)), dma((L, n, C)), dma((L, na, C)),
        ],
        compiler_params=pltpu.CompilerParams(
            collective_id=0, has_side_effects=True, vmem_limit_bytes=40 * 1024 * 1024),
    )(prompt.reshape(n, tb, D), norm_gain[:, :, None], gate_weight, up_weight, down_weight)
    gate, up, down, mixed = pl.pallas_call(
        write_out,
        out_shape=(
            jax.ShapeDtypeStruct((L, n, R, FFb), bf16),
            jax.ShapeDtypeStruct((L, n, R, FFb), bf16),
            jax.ShapeDtypeStruct((L, FFb, D), bf16),
            jax.ShapeDtypeStruct((n, tb, D), bf16),
        ),
        in_specs=[anym] * 3,
        out_specs=(anym,) * 4,
        scratch_shapes=[dma((L, 2)), dma((L, G * T)), dma(())],
        compiler_params=pltpu.CompilerParams(vmem_limit_bytes=1024 * 1024),
    )(*(pltpu.with_memory_space_constraint(x, pltpu.VMEM) for x in (wall, dn, ag)))
    return (gate.reshape(L, n * R, FFb), up.reshape(L, n * R, FFb), down, mixed.reshape(prompt.shape))


def solution(mesh):
    G, n, T = mesh.shape["gr"], mesh.shape["fs"], mesh.shape["tp"]
    in_specs = (
        P(("gr", "tp"), None, None),
        P(None, "fs"),
        P(None, "fs", ("gr", "tp")),
        P(None, "fs", ("gr", "tp")),
        P(None, "fs", ("gr", "tp")),
    )
    out_specs = (
        P(None, None, "fs"),
        P(None, None, "fs"),
        P(None, "fs", None),
        P(("gr", "tp"), None, None),
    )
    return jax.shard_map(
        functools.partial(per_device, G, n, T),
        mesh=mesh, in_specs=in_specs, out_specs=out_specs, check_vma=False)
```

```python
import functools

import jax
import jax.numpy as jnp
from jax import lax
from jax.experimental import pallas as pl
from jax.experimental.pallas import tpu as pltpu
from jax.sharding import PartitionSpec as P

norm_eps = 1e-06
MESH = pl.DeviceIdType.MESH
f32 = jnp.float32
bf16 = jnp.bfloat16


def kernel(G, n, T, prompt_h, gain_h, gate_h, up_h, down_h,
           wall, dn, ag,
           prompt, gain, gate_w, up_w, down_w, in_s, wsrc, p, r1, q2, r2, r3, sums, lhs, hid, st,
           x_s, x_r, v_s, v_r, xd_s, p_s, w_r, w_l, f_s, d_s, d_r,
           s1_s, s1_r, s2_s, s2_r, s3_s, s3_r, g_s, gg_s, g_r, h_s):
    gr, fs, tp = lax.axis_index("gr"), lax.axis_index("fs"), lax.axis_index("tp")
    q, R, FFb = wsrc.shape[3:]
    tb, D = prompt.shape[1:]
    rows = n * tb
    DC = dn.shape[3]
    na = n // 2
    wing = n // 2 if n % 2 == 0 else n
    a, b = fs // 2, lax.rem(fs, 2)
    C = s1_s.shape[2]
    tc = tb // C
    peer = fs + 1 - 2 * b
    is_recv = lax.rem(fs // q, T) == tp
    slot_me = gr * T + tp
    hs = [(R * c // 16) // 16 * 16 if G == 2 else 0 for c in (4, 8)]

    def mine(k, g):
        return pl.ds(pl.multiple_of(g * hs[k], 16), R - hs[k]) if hs[k] else pl.ds(0, R)

    def only(k, g):
        return pl.ds(pl.multiple_of(g * (R - hs[k]), 16), hs[k])

    def dev(g, f, t):
        return {"gr": g, "fs": f, "tp": t}

    def rc(src, dst, ss, rs, d):
        return pltpu.make_async_remote_copy(
            src_ref=src, dst_ref=dst, send_sem=ss, recv_sem=rs,
            device_id=d, device_id_type=MESH)

    def loop(lo, hi, body):
        def step(i, c):
            body(i)
            return c
        lax.fori_loop(lo, hi, step, 0)

    turn = [lax.rem(i + b + 1, q) for i in range(q)]
    others_g = [lax.rem(gr + d, G) for d in range(1, G)]
    loads = [pltpu.make_async_copy(gain_h, gain, in_s.at[0])]
    for k in range(2):
        for h, v in ((gate_h, gate_w), (up_h, up_w), (down_h, down_w)):
            loads.append(pltpu.make_async_copy(h.at[k], v.at[k], in_s.at[len(loads)]))
    loads.append(pltpu.make_async_copy(prompt_h, prompt, in_s.at[len(loads)]))
    others_t = [lax.rem(tp + d, T) for d in range(1, T)]

    def x_copy(k, w, i, g_src, g_dst):
        blk = wsrc.at[k, w, g_src, i, mine(k, g_dst)]
        return rc(blk, blk, x_s.at[k, w, i, g_dst], x_r.at[k, w, i, g_src], dev(g_dst, fs, tp))

    def xd_copy(k, g_src, g_dst):
        blk = dn.at[k, g_src * T + tp]
        return rc(blk, blk, xd_s.at[k, g_dst], d_r.at[k, g_src * T + tp], dev(g_dst, fs, tp))

    def d_copy(k, g_src, t_src, t_dst):
        blk = dn.at[k, g_src * T + t_src]
        return rc(blk, blk, d_s.at[k, g_src, t_dst], d_r.at[k, g_src * T + t_src], dev(gr, fs, t_dst))

    def col_of(g, i):
        return (g * T + tp) * q + i

    def p_copy(k, w, g, i):
        return rc(wsrc.at[k, w, g, i, mine(k, gr)], wall.at[k, w, fs, mine(k, gr)], p_s.at[k, w, g, i],
                  w_r.at[k, w, fs], dev(gr, col_of(g, i), tp))

    def l_copy(k, w, g, i):
        return pltpu.make_async_copy(wsrc.at[k, w, g, i, mine(k, gr)], wall.at[k, w, fs, mine(k, gr)], w_l.at[k, w])

    def f_copy(k, w, f, t):
        blk = wall.at[k, w, f, mine(k, gr)]
        return rc(blk, blk, f_s.at[k, w, 0, f, t], w_r.at[k, w, f], dev(gr, fs, t))

    def v_copy(k, w, f, g_src):
        blk = wall.at[k, w, f, only(k, g_src)]
        return rc(blk, blk, v_s.at[k, w, f], v_r.at[k, w, 0, f], dev(1 - g_src, fs, tp))

    def fv_copy(k, w, f, t):
        blk = wall.at[k, w, f, only(k, 1 - gr)]
        return rc(blk, blk, f_s.at[k, w, 1, f, t], v_r.at[k, w, 1, f], dev(gr, fs, t))

    def column(k):
        eye = lax.broadcasted_iota(jnp.int32, (R, R), 0) == lax.broadcasted_iota(jnp.int32, (R, R), 1)
        return jnp.sum(jnp.where(eye, gain[k:k + 1], 0.0), axis=1, keepdims=True)

    def cast_w(k, w):
        ref = (gate_w, up_w)[w]
        loads[1 + 3 * k + w].wait()
        for i in range(q):
            wsrc[k, w, gr, i] = (column(k) * ref[k, :, i * FFb:(i + 1) * FFb]).astype(bf16)

    def xsend_w(k, w):
        for i in turn:
            for g in others_g:
                x_copy(k, w, i, gr, g).start()

    def cast_d(k):
        loads[3 + 3 * k].wait()
        dn[k, slot_me] = down_w[k].astype(bf16)

    def xsend_d(k):
        for g in others_g:
            xd_copy(k, gr, g).start()
        for t in others_t:
            d_copy(k, gr, tp, t).start()

    def plane(k, w, g, i):
        c = col_of(g, i)

        @pl.when(c != fs)
        def _():
            p_copy(k, w, g, i).start()

        @pl.when(c == fs)
        def _():
            l_copy(k, w, g, i).start()

    def plane_own(k, w):
        for i in turn:
            plane(k, w, gr, i)

    def plane_x(k, w):
        for g in others_g:
            for i in turn:
                x_copy(k, w, i, g, gr).wait_recv()
                plane(k, w, g, i)

    def source(s):
        e = s // wing
        return lax.rem((fs // wing + e) * wing + lax.rem(fs + s, wing), n)

    def arrive(k, w):
        def forward(f):
            for t in others_t:
                f_copy(k, w, f, t).start()
            if hs[k]:
                v_copy(k, w, f, gr).start()

        @pl.when(is_recv)
        def _():
            l_copy(k, w, 0, 0).wait()
            forward(fs)

            def take(s):
                f = source(s)
                f_copy(k, w, f, tp).wait_recv()
                forward(f)
            loop(1, n, take)

    def cross(k, w):
        if hs[k]:
            @pl.when(is_recv)
            def _():
                def take(s):
                    f = source(s)
                    v_copy(k, w, f, 1 - gr).wait_recv()
                    for t in others_t:
                        fv_copy(k, w, f, t).start()
                loop(0, n, take)

    def landed(k, w):
        @pl.when(jnp.logical_not(is_recv))
        def _():
            def take(f):
                f_copy(k, w, f, tp).wait_recv()
                if hs[k]:
                    fv_copy(k, w, f, tp).wait_recv()
            loop(0, n, take)

    def relay_d(k):
        for g in others_g:
            xd_copy(k, g, gr).wait_recv()
            for t in others_t:
                d_copy(k, g, tp, t).start()

    def landed_d(k):
        for g in range(G):
            for t in others_t:
                d_copy(k, g, t, tp).wait_recv()

    def gather_done(k):
        for w in range(2):
            for i in range(q):
                for g in others_g:
                    x_copy(k, w, i, gr, g).wait_send()
            for g in range(G):
                for i in range(q):
                    @pl.when(col_of(g, i) != fs)
                    def _():
                        p_copy(k, w, g, i).wait_send()

            @pl.when(is_recv)
            def _():
                def sent(f):
                    for t in others_t:
                        f_copy(k, w, f, t).wait_send()
                        if hs[k]:
                            fv_copy(k, w, f, t).wait_send()
                    if hs[k]:
                        v_copy(k, w, f, gr).wait_send()
                loop(0, n, sent)
        for g in others_g:
            xd_copy(k, gr, g).wait_send()
        for g in range(G):
            for t in others_t:
                d_copy(k, g, tp, t).wait_send()

    def flatten(ref):
        cw = 256

        def chunk(j):
            cols = pl.ds(pl.multiple_of(j * cw, cw), cw)
            lhs[:, cols] = ref[:, :, cols].astype(f32).reshape(rows, cw).astype(bf16)
        loop(0, D // cw, chunk)

    def normed_of(x):
        return (x * lax.rsqrt(jnp.mean(x * x, axis=-1, keepdims=True) + norm_eps)).astype(bf16)

    def compute(k):
        ft = min(FFb, 256)

        def act(j):
            cols = pl.ds(pl.multiple_of(j * ft, ft), ft)
            gate = jnp.dot(lhs[...], wall[k, 0, :, :, cols].reshape(D, ft), preferred_element_type=f32)
            up = jnp.dot(lhs[...], wall[k, 1, :, :, cols].reshape(D, ft), preferred_element_type=f32)
            hid[:, cols] = (gate / (1.0 + jnp.exp(-gate)) * up).astype(bf16)
        loop(0, FFb // ft, act)

        def proj(s):
            cols = pl.ds(pl.multiple_of(s * DC, DC), DC)
            v = jnp.dot(hid[...], dn[k, s], preferred_element_type=f32)
            p[k, :, :, cols] = v.reshape(n, tb, DC).astype(bf16)
        loop(0, G * T, proj)

    half = na // 2 if na % 2 == 0 else na
    far = na // half - 1
    pos = lax.rem(a, half)
    mirror = lax.rem(a + half, na)

    def near(d):
        return a - pos + lax.rem(pos + d, half)

    def across(a2):
        return lax.rem(a2 + half, na)

    def part(c):
        return pl.ds(c * tc, tc)

    def s1_copy(k, a2, c):
        return rc(p.at[k, 2 * a2 + 1 - b, part(c)], r1.at[k, a2, part(c)],
                  s1_s.at[k, a2, c], s1_r.at[k, a2, c], dev(gr, peer, tp))

    def s2_copy(k, a2, a_from, c):
        return rc(q2.at[k, a2, part(c)], r2.at[k, a_from, part(c)],
                  s2_s.at[k, a2, c], s2_r.at[k, a_from, c], dev(gr, 2 * a2 + b, tp))

    def s3_copy(k, o, a_from, c):
        return rc(q2.at[k, across(o), part(c)], r3.at[k, a_from, part(c)],
                  s3_s.at[k, o, c], s3_r.at[k, a_from, c], dev(gr, 2 * o + b, tp))

    def rs_first(k):
        for c in range(C):
            if far:
                def send_far(d):
                    s1_copy(k, across(near(d)), c).start()
                loop(1, half, send_far)

            def send(d):
                s1_copy(k, near(d), c).start()
            loop(1, half, send)
            if far:
                s1_copy(k, mirror, c).start()
            s1_copy(k, a, c).start()

    def pair(k, a2, c):
        s1_copy(k, a2, c).wait_recv()
        return p[k, 2 * a2 + b, part(c)].astype(f32) + r1[k, a2, part(c)].astype(f32)

    def rs_remote(k, c):
        if far:
            def help_far(d):
                o = near(d)
                q2[k, across(o), part(c)] = pair(k, across(o), c).astype(bf16)
                s3_copy(k, o, a, c).start()
            loop(1, half, help_far)

        def send(d):
            o = near(d)
            q2[k, o, part(c)] = pair(k, o, c).astype(bf16)
            s2_copy(k, o, a, c).start()
        loop(1, half, send)

    def rs_mid(k, c):
        if far:
            sums[part(c)] = pair(k, mirror, c)

            def take(d):
                o = near(d)
                s3_copy(k, a, o, c).wait_recv()
                sums[part(c)] += r3[k, o, part(c)].astype(f32)
            loop(1, half, take)
            q2[k, mirror, part(c)] = sums[part(c)].astype(bf16)
            s2_copy(k, mirror, a, c).start()

    def rs_own(k, c):
        st[part(c)] += 0.5 * pair(k, a, c)

    def rs_last(k, c):
        def take(a2):
            s2_copy(k, a2, a2, c).wait_recv()
            st[part(c)] += 0.5 * r2[k, a2, part(c)].astype(f32)
        loop(1, half, lambda d: take(near(d)))
        if far:
            take(mirror)
        x = st[part(c)]
        ag[k, fs, part(c)] = normed_of(x) if k == 0 else x.astype(bf16)

        if far:
            z_copy(k, fs, mirror, c).start()

        def send(d):
            z_copy(k, fs, near(d), c).start()
        loop(1, half, send)
        y_copy(k, fs, c).start()

    def z_copy(k, j, a2, c):
        blk = ag.at[k, j, part(c)]
        return rc(blk, blk, g_s.at[k, a2, c], g_r.at[k, j, c], dev(gr, 2 * a2 + b, tp))

    def y_copy(k, j, c):
        blk = ag.at[k, j, part(c)]
        return rc(blk, blk, h_s.at[k, j // 2, c], g_r.at[k, j, c], dev(gr, peer, tp))

    def zz_copy(k, a2, c):
        blk = ag.at[k, 2 * mirror + b, part(c)]
        return rc(blk, blk, gg_s.at[k, a2, c], g_r.at[k, 2 * mirror + b, c], dev(gr, 2 * a2 + b, tp))

    def pass_on(k, a2, c):
        z_copy(k, 2 * a2 + b, a2, c).wait_recv()
        y_copy(k, 2 * a2 + b, c).start()

    def ag_pass(k, c):
        def own(d):
            pass_on(k, near(d), c)
        loop(1, half, own)
        if far:
            z_copy(k, 2 * mirror + b, a, c).wait_recv()

            def spread(d):
                zz_copy(k, near(d), c).start()
            loop(1, half, spread)
            y_copy(k, 2 * mirror + b, c).start()

    def ag_far(k, c):
        if far:
            def theirs(d):
                pass_on(k, across(near(d)), c)
            loop(1, half, theirs)

    def ag_take(k):
        for c in range(C):
            def take(a2):
                y_copy(k, 2 * a2 + 1 - b, c).wait_recv()
            loop(0, na, take)

    def rs_done(k):
        for c in range(C):
            def sent(a2):
                s1_copy(k, a2, c).wait_send()
            loop(0, na, sent)

            def sent2(d):
                s2_copy(k, near(d), a, c).wait_send()
                if far:
                    s3_copy(k, near(d), a, c).wait_send()
            loop(1, half, sent2)
            if far:
                s2_copy(k, mirror, a, c).wait_send()

    def ag_done(k):
        for c in range(C):
            def sent(d):
                z_copy(k, fs, near(d), c).wait_send()
                if far:
                    zz_copy(k, near(d), c).wait_send()
            loop(1, half, sent)
            if far:
                z_copy(k, fs, mirror, c).wait_send()

            def sent2(a2):
                y_copy(k, 2 * a2 + b, c).wait_send()
            loop(0, na, sent2)

    for load in loads:
        load.start()
    barrier = pltpu.get_barrier_semaphore()

    def greet(s):
        pl.semaphore_signal(barrier, inc=1, device_id=dev(gr, lax.rem(fs + s, n), tp), device_id_type=MESH)
    loop(1, n, greet)
    for t in others_t:
        pl.semaphore_signal(barrier, inc=1, device_id=dev(gr, fs, t), device_id_type=MESH)
    for g in others_g:
        pl.semaphore_signal(barrier, inc=1, device_id=dev(g, fs, tp), device_id_type=MESH)
    loads[0].wait()
    cast_w(0, 0)
    pl.semaphore_wait(barrier, n + T + G - 3)

    def norm_rows(j):
        p[0, j] = normed_of(prompt[j].astype(f32))

    def start_tokens():
        loads[7].wait()
        loop(0, n, norm_rows)
        flatten(p.at[0])
        st[...] = prompt[fs].astype(f32)

    def unpack(k):
        flatten(ag.at[k])

    def done(k):
        gather_done(k)
        rs_done(k)
        ag_done(k)

    xsend_w(0, 0)
    plane_own(0, 0)
    cast_w(0, 1)
    xsend_w(0, 1)
    plane_own(0, 1)
    cast_d(0)
    xsend_d(0)
    cast_w(1, 0)
    cast_w(1, 1)
    cast_d(1)
    start_tokens()
    xsend_w(1, 0)
    plane_x(0, 0)
    plane_x(0, 1)
    arrive(0, 0)
    arrive(0, 1)
    relay_d(0)
    cross(0, 0)
    landed(0, 0)
    xsend_w(1, 1)
    plane_own(1, 0)
    plane_x(1, 0)
    cross(0, 1)
    landed(0, 1)
    plane_own(1, 1)
    landed_d(0)
    compute(0)
    rs_first(0)
    plane_x(1, 1)
    xsend_d(1)
    rs_remote(0, 0)
    arrive(1, 0)
    rs_mid(0, 0)
    rs_own(0, 0)
    if C > 1:
        rs_remote(0, 1)
        rs_last(0, 0)
        rs_mid(0, 1)
        rs_own(0, 1)
    arrive(1, 1)
    rs_last(0, C - 1)
    relay_d(1)
    ag_pass(0, 0)
    ag_far(0, 0)
    if C > 1:
        ag_pass(0, 1)
        ag_far(0, 1)
    cross(1, 0)
    cross(1, 1)
    ag_take(0)
    unpack(0)
    landed(1, 0)
    landed(1, 1)
    landed_d(1)
    compute(1)
    rs_first(1)
    rs_remote(1, 0)
    rs_mid(1, 0)
    rs_own(1, 0)
    if C > 1:
        rs_remote(1, 1)
        rs_last(1, 0)
        rs_mid(1, 1)
        rs_own(1, 1)
        ag_pass(1, 0)
    rs_last(1, C - 1)
    if C == 1:
        ag_pass(1, 0)
    ag_far(1, 0)
    if C > 1:
        ag_pass(1, 1)
        ag_far(1, 1)
    ag_take(1)
    done(0)
    done(1)


def write_out(wall, dn, ag, gate_o, up_o, down_o, mixed_o, o_s, d_s, m_s):
    L, S, _, DC = dn.shape
    copies = []
    for k in range(L):
        copies.append(pltpu.make_async_copy(wall.at[k, 0], gate_o.at[k], o_s.at[k, 0]))
        copies.append(pltpu.make_async_copy(wall.at[k, 1], up_o.at[k], o_s.at[k, 1]))
        for s in range(S):
            copies.append(pltpu.make_async_copy(
                dn.at[k, s], down_o.at[k, :, pl.ds(s * DC, DC)], d_s.at[k, s]))
    copies.append(pltpu.make_async_copy(ag.at[L - 1], mixed_o, m_s))
    for c in copies:
        c.start()
    for c in copies:
        c.wait()


def per_device(G, n, T, prompt, norm_gain, gate_weight, up_weight, down_weight):
    D = prompt.shape[2]
    rows = prompt.shape[0] * prompt.shape[1]
    L, R, C_ = gate_weight.shape
    FFb, DC = down_weight.shape[1:]
    q = C_ // FFb
    tb = rows // n
    na = n // 2
    C = max(1, min(2, tb // 8))
    dma = pltpu.SemaphoreType.DMA
    vmem = pl.BlockSpec(memory_space=pltpu.VMEM)
    anym = pl.BlockSpec(memory_space=pl.ANY)
    wall, dn, ag = pl.pallas_call(
        functools.partial(kernel, G, n, T),
        out_shape=(
            pltpu.VMEM((L, 2, n, R, FFb), bf16),
            pltpu.VMEM((L, G * T, FFb, DC), bf16),
            pltpu.VMEM((L, n, tb, D), bf16),
        ),
        in_specs=[pl.BlockSpec(memory_space=pltpu.HBM)] * 5,
        out_specs=(vmem,) * 3,
        scratch_shapes=[
            pltpu.VMEM((n, tb, D), bf16), pltpu.VMEM((L, R), f32),
            pltpu.VMEM((L, R, C_), f32), pltpu.VMEM((L, R, C_), f32), pltpu.VMEM((L, FFb, DC), f32),
            dma((8,)),
            pltpu.VMEM((L, 2, G, q, R, FFb), bf16),
            pltpu.VMEM((L, n, tb, D), bf16),
            pltpu.VMEM((L, na, tb, D), bf16),
            pltpu.VMEM((L, na, tb, D), bf16),
            pltpu.VMEM((L, na, tb, D), bf16),
            pltpu.VMEM((L, na, tb, D), bf16),
            pltpu.VMEM((tb, D), f32),
            pltpu.VMEM((rows, D), bf16),
            pltpu.VMEM((rows, FFb), bf16),
            pltpu.VMEM((tb, D), f32),
            dma((L, 2, q, G)), dma((L, 2, q, G)), dma((L, 2, n)), dma((L, 2, 2, n)), dma((L, G)),
            dma((L, 2, G, q)), dma((L, 2, n)), dma((L, 2)), dma((L, 2, 2, n, T)),
            dma((L, G, T)), dma((L, G * T)),
            dma((L, na, C)), dma((L, na, C)), dma((L, na, C)), dma((L, na, C)), dma((L, na, C)), dma((L, na, C)),
            dma((L, na, C)), dma((L, na, C)), dma((L, n, C)), dma((L, na, C)),
        ],
        compiler_params=pltpu.CompilerParams(
            collective_id=0, has_side_effects=True, vmem_limit_bytes=40 * 1024 * 1024),
    )(prompt.reshape(n, tb, D), norm_gain, gate_weight, up_weight, down_weight)
    gate, up, down, mixed = pl.pallas_call(
        write_out,
        out_shape=(
            jax.ShapeDtypeStruct((L, n, R, FFb), bf16),
            jax.ShapeDtypeStruct((L, n, R, FFb), bf16),
            jax.ShapeDtypeStruct((L, FFb, D), bf16),
            jax.ShapeDtypeStruct((n, tb, D), bf16),
        ),
        in_specs=[anym] * 3,
        out_specs=(anym,) * 4,
        scratch_shapes=[dma((L, 2)), dma((L, G * T)), dma(())],
        compiler_params=pltpu.CompilerParams(vmem_limit_bytes=1024 * 1024),
    )(*(pltpu.with_memory_space_constraint(x, pltpu.VMEM) for x in (wall, dn, ag)))
    return (gate.reshape(L, n * R, FFb), up.reshape(L, n * R, FFb), down, mixed.reshape(prompt.shape))


def solution(mesh):
    G, n, T = mesh.shape["gr"], mesh.shape["fs"], mesh.shape["tp"]
    in_specs = (
        P(("gr", "tp"), None, None),
        P(None, "fs"),
        P(None, "fs", ("gr", "tp")),
        P(None, "fs", ("gr", "tp")),
        P(None, "fs", ("gr", "tp")),
    )
    out_specs = (
        P(None, None, "fs"),
        P(None, None, "fs"),
        P(None, "fs", None),
        P(("gr", "tp"), None, None),
    )
    return jax.shard_map(
        functools.partial(per_device, G, n, T),
        mesh=mesh, in_specs=in_specs, out_specs=out_specs, check_vma=False)
```

```python
import functools

import jax
import jax.numpy as jnp
from jax import lax
from jax.experimental import pallas as pl
from jax.experimental.pallas import tpu as pltpu
from jax.sharding import PartitionSpec as P

norm_eps = 1e-06
MESH = pl.DeviceIdType.MESH
f32 = jnp.float32
bf16 = jnp.bfloat16


def kernel(G, n, T, prompt_h, gain_h, gate_h, up_h, down_h,
           wall, dn, ag,
           prompt, gain, gate_w, up_w, down_w, in_s, wsrc, p, r1, q2, r2, r3, sums, lhs, hid, gact, st,
           x_s, x_r, v_s, v_r, xd_s, p_s, w_r, w_l, f_s, d_s, d_r,
           s1_s, s1_r, s2_s, s2_r, s3_s, s3_r, g_s, gg_s, g_r, h_s):
    gr, fs, tp = lax.axis_index("gr"), lax.axis_index("fs"), lax.axis_index("tp")
    q, R, FFb = wsrc.shape[3:]
    tb, D = prompt.shape[1:]
    rows = n * tb
    DC = dn.shape[3]
    na = n // 2
    wing = n // 2 if n % 2 == 0 else n
    a, b = fs // 2, lax.rem(fs, 2)
    C = s1_s.shape[2]
    tc = tb // C
    peer = fs + 1 - 2 * b
    is_recv = lax.rem(fs // q, T) == tp
    slot_me = gr * T + tp
    hs = [(R * c // 16) // 16 * 16 if G == 2 else 0 for c in (4, 8)]

    def mine(k, g):
        return pl.ds(pl.multiple_of(g * hs[k], 16), R - hs[k]) if hs[k] else pl.ds(0, R)

    def only(k, g):
        return pl.ds(pl.multiple_of(g * (R - hs[k]), 16), hs[k])

    def dev(g, f, t):
        return {"gr": g, "fs": f, "tp": t}

    def rc(src, dst, ss, rs, d):
        return pltpu.make_async_remote_copy(
            src_ref=src, dst_ref=dst, send_sem=ss, recv_sem=rs,
            device_id=d, device_id_type=MESH)

    def loop(lo, hi, body):
        def step(i, c):
            body(i)
            return c
        lax.fori_loop(lo, hi, step, 0)

    turn = [lax.rem(i + b + 1, q) for i in range(q)]
    others_g = [lax.rem(gr + d, G) for d in range(1, G)]
    loads = [pltpu.make_async_copy(gain_h, gain, in_s.at[0])]
    for k in range(2):
        for h, v in ((gate_h, gate_w), (up_h, up_w), (down_h, down_w)):
            loads.append(pltpu.make_async_copy(h.at[k], v.at[k], in_s.at[len(loads)]))
    loads.append(pltpu.make_async_copy(prompt_h, prompt, in_s.at[len(loads)]))
    others_t = [lax.rem(tp + d, T) for d in range(1, T)]

    def x_copy(k, w, i, g_src, g_dst):
        blk = wsrc.at[k, w, g_src, i, mine(k, g_dst)]
        return rc(blk, blk, x_s.at[k, w, i, g_dst], x_r.at[k, w, i, g_src], dev(g_dst, fs, tp))

    def xd_copy(k, g_src, g_dst):
        blk = dn.at[k, g_src * T + tp]
        return rc(blk, blk, xd_s.at[k, g_dst], d_r.at[k, g_src * T + tp], dev(g_dst, fs, tp))

    def d_copy(k, g_src, t_src, t_dst):
        blk = dn.at[k, g_src * T + t_src]
        return rc(blk, blk, d_s.at[k, g_src, t_dst], d_r.at[k, g_src * T + t_src], dev(gr, fs, t_dst))

    def col_of(g, i):
        return (g * T + tp) * q + i

    def p_copy(k, w, g, i):
        return rc(wsrc.at[k, w, g, i, mine(k, gr)], wall.at[k, w, fs, mine(k, gr)], p_s.at[k, w, g, i],
                  w_r.at[k, w, fs], dev(gr, col_of(g, i), tp))

    def l_copy(k, w, g, i):
        return pltpu.make_async_copy(wsrc.at[k, w, g, i, mine(k, gr)], wall.at[k, w, fs, mine(k, gr)], w_l.at[k, w])

    def f_copy(k, w, f, t):
        blk = wall.at[k, w, f, mine(k, gr)]
        return rc(blk, blk, f_s.at[k, w, 0, f, t], w_r.at[k, w, f], dev(gr, fs, t))

    def v_copy(k, w, f, g_src):
        blk = wall.at[k, w, f, only(k, g_src)]
        return rc(blk, blk, v_s.at[k, w, f], v_r.at[k, w, 0, f], dev(1 - g_src, fs, tp))

    def fv_copy(k, w, f, t):
        blk = wall.at[k, w, f, only(k, 1 - gr)]
        return rc(blk, blk, f_s.at[k, w, 1, f, t], v_r.at[k, w, 1, f], dev(gr, fs, t))

    def column(k):
        eye = lax.broadcasted_iota(jnp.int32, (R, R), 0) == lax.broadcasted_iota(jnp.int32, (R, R), 1)
        return jnp.sum(jnp.where(eye, gain[k:k + 1], 0.0), axis=1, keepdims=True)

    def cast_w(k, w):
        ref = (gate_w, up_w)[w]
        loads[1 + 3 * k + w].wait()
        for i in range(q):
            wsrc[k, w, gr, i] = (column(k) * ref[k, :, i * FFb:(i + 1) * FFb]).astype(bf16)

    def xsend_w(k, w):
        for i in turn:
            for g in others_g:
                x_copy(k, w, i, gr, g).start()

    def cast_d(k):
        loads[3 + 3 * k].wait()
        dn[k, slot_me] = down_w[k].astype(bf16)

    def xsend_d(k):
        for g in others_g:
            xd_copy(k, gr, g).start()
        for t in others_t:
            d_copy(k, gr, tp, t).start()

    def plane(k, w, g, i):
        c = col_of(g, i)

        @pl.when(c != fs)
        def _():
            p_copy(k, w, g, i).start()

        @pl.when(c == fs)
        def _():
            l_copy(k, w, g, i).start()

    def plane_own(k, w):
        for i in turn:
            plane(k, w, gr, i)

    def plane_x(k, w):
        for g in others_g:
            for i in turn:
                x_copy(k, w, i, g, gr).wait_recv()
                plane(k, w, g, i)

    def source(s):
        e = s // wing
        return lax.rem((fs // wing + e) * wing + lax.rem(fs + s, wing), n)

    def arrive(k, w):
        def forward(f):
            for t in others_t:
                f_copy(k, w, f, t).start()
            if hs[k]:
                v_copy(k, w, f, gr).start()

        @pl.when(is_recv)
        def _():
            l_copy(k, w, 0, 0).wait()
            forward(fs)

            def take(s):
                f = source(s)
                f_copy(k, w, f, tp).wait_recv()
                forward(f)
            loop(1, n, take)

    def cross(k, w):
        if hs[k]:
            @pl.when(is_recv)
            def _():
                def take(s):
                    f = source(s)
                    v_copy(k, w, f, 1 - gr).wait_recv()
                    for t in others_t:
                        fv_copy(k, w, f, t).start()
                loop(0, n, take)

    def landed(k, w):
        @pl.when(jnp.logical_not(is_recv))
        def _():
            def take(f):
                f_copy(k, w, f, tp).wait_recv()
                if hs[k]:
                    fv_copy(k, w, f, tp).wait_recv()
            loop(0, n, take)

    def relay_d(k):
        for g in others_g:
            xd_copy(k, g, gr).wait_recv()
            for t in others_t:
                d_copy(k, g, tp, t).start()

    def landed_d(k):
        for g in range(G):
            for t in others_t:
                d_copy(k, g, t, tp).wait_recv()

    def gather_done(k):
        for w in range(2):
            for i in range(q):
                for g in others_g:
                    x_copy(k, w, i, gr, g).wait_send()
            for g in range(G):
                for i in range(q):
                    @pl.when(col_of(g, i) != fs)
                    def _():
                        p_copy(k, w, g, i).wait_send()

            @pl.when(is_recv)
            def _():
                def sent(f):
                    for t in others_t:
                        f_copy(k, w, f, t).wait_send()
                        if hs[k]:
                            fv_copy(k, w, f, t).wait_send()
                    if hs[k]:
                        v_copy(k, w, f, gr).wait_send()
                loop(0, n, sent)
        for g in others_g:
            xd_copy(k, gr, g).wait_send()
        for g in range(G):
            for t in others_t:
                d_copy(k, g, tp, t).wait_send()

    def flatten(ref):
        cw = 256

        def chunk(j):
            cols = pl.ds(pl.multiple_of(j * cw, cw), cw)
            lhs[:, cols] = ref[:, :, cols].astype(f32).reshape(rows, cw).astype(bf16)
        loop(0, D // cw, chunk)

    def normed_of(x):
        return (x * lax.rsqrt(jnp.mean(x * x, axis=-1, keepdims=True) + norm_eps)).astype(bf16)

    def gates(k):
        ft = min(FFb, 256)

        def act(j):
            cols = pl.ds(j * ft, ft)
            gact[:, cols] = jnp.dot(lhs[...], wall[k, 0, :, :, cols].reshape(D, ft), preferred_element_type=f32)
        for j in range(FFb // ft):
            act(j)

    def compute(k):
        ft = min(FFb, 256)

        def act(j):
            cols = pl.ds(j * ft, ft)
            gate = gact[:, cols]
            up = jnp.dot(lhs[...], wall[k, 1, :, :, cols].reshape(D, ft), preferred_element_type=f32)
            hid[:, cols] = (gate / (1.0 + jnp.exp(-gate)) * up).astype(bf16)
        for j in range(FFb // ft):
            act(j)

        def proj(s):
            cols = pl.ds(s * DC, DC)
            v = jnp.dot(hid[...], dn[k, s], preferred_element_type=f32)
            p[k, :, :, cols] = v.reshape(n, tb, DC).astype(bf16)
        for s in range(G * T):
            proj(s)

    half = na // 2 if na % 2 == 0 else na
    far = na // half - 1
    pos = lax.rem(a, half)
    mirror = lax.rem(a + half, na)

    def near(d):
        return a - pos + lax.rem(pos + d, half)

    def across(a2):
        return lax.rem(a2 + half, na)

    def part(c):
        return pl.ds(c * tc, tc)

    def s1_copy(k, a2, c):
        return rc(p.at[k, 2 * a2 + 1 - b, part(c)], r1.at[k, a2, part(c)],
                  s1_s.at[k, a2, c], s1_r.at[k, a2, c], dev(gr, peer, tp))

    def s2_copy(k, a2, a_from, c):
        return rc(q2.at[k, a2, part(c)], r2.at[k, a_from, part(c)],
                  s2_s.at[k, a2, c], s2_r.at[k, a_from, c], dev(gr, 2 * a2 + b, tp))

    def s3_copy(k, o, a_from, c):
        return rc(q2.at[k, across(o), part(c)], r3.at[k, a_from, part(c)],
                  s3_s.at[k, o, c], s3_r.at[k, a_from, c], dev(gr, 2 * o + b, tp))

    def rs_first(k):
        def send(of):
            def chunks(d):
                for c in range(C):
                    s1_copy(k, of(d), c).start()
            return chunks
        if far:
            loop(1, half, send(lambda d: across(near(d))))
            send(lambda d: mirror)(0)
        loop(1, half, send(near))
        send(lambda d: a)(0)

    def pair(k, a2, c):
        s1_copy(k, a2, c).wait_recv()
        return p[k, 2 * a2 + b, part(c)].astype(f32) + r1[k, a2, part(c)].astype(f32)

    def rs_far(k, c):
        if far:
            def send(d):
                o = near(d)
                q2[k, across(o), part(c)] = pair(k, across(o), c).astype(bf16)
                s3_copy(k, o, a, c).start()
            loop(1, half, send)

    def rs_near(k, c):
        def send(d):
            o = near(d)
            q2[k, o, part(c)] = pair(k, o, c).astype(bf16)
            s2_copy(k, o, a, c).start()
        loop(1, half, send)

    def rs_mid(k, c):
        if far:
            sums[part(c)] = pair(k, mirror, c)

            def take(d):
                o = near(d)
                s3_copy(k, a, o, c).wait_recv()
                sums[part(c)] += r3[k, o, part(c)].astype(f32)
            loop(1, half, take)
            q2[k, mirror, part(c)] = sums[part(c)].astype(bf16)
            s2_copy(k, mirror, a, c).start()

    def rs_own(k, c):
        st[part(c)] += 0.5 * pair(k, a, c)

    def rs_last(k, c):
        def take(a2):
            s2_copy(k, a2, a2, c).wait_recv()
            st[part(c)] += 0.5 * r2[k, a2, part(c)].astype(f32)
        loop(1, half, lambda d: take(near(d)))
        if far:
            take(mirror)
        x = st[part(c)]
        ag[k, fs, part(c)] = normed_of(x) if k == 0 else x.astype(bf16)

        if far:
            z_copy(k, fs, mirror, c).start()

        def send(d):
            z_copy(k, fs, near(d), c).start()
        loop(1, half, send)
        y_copy(k, fs, c).start()

    def z_copy(k, j, a2, c):
        blk = ag.at[k, j, part(c)]
        return rc(blk, blk, g_s.at[k, a2, c], g_r.at[k, j, c], dev(gr, 2 * a2 + b, tp))

    def y_copy(k, j, c):
        blk = ag.at[k, j, part(c)]
        return rc(blk, blk, h_s.at[k, j // 2, c], g_r.at[k, j, c], dev(gr, peer, tp))

    def zz_copy(k, a2, c):
        blk = ag.at[k, 2 * mirror + b, part(c)]
        return rc(blk, blk, gg_s.at[k, a2, c], g_r.at[k, 2 * mirror + b, c], dev(gr, 2 * a2 + b, tp))

    def pass_on(k, a2, c):
        z_copy(k, 2 * a2 + b, a2, c).wait_recv()
        y_copy(k, 2 * a2 + b, c).start()

    def ag_pass(k, c):
        def own(d):
            pass_on(k, near(d), c)
        loop(1, half, own)
        if far:
            z_copy(k, 2 * mirror + b, a, c).wait_recv()

            def spread(d):
                zz_copy(k, near(d), c).start()
            loop(1, half, spread)
            y_copy(k, 2 * mirror + b, c).start()

    def ag_far(k, c):
        if far:
            def theirs(d):
                pass_on(k, across(near(d)), c)
            loop(1, half, theirs)

    def ag_take(k):
        for c in range(C):
            def take(a2):
                y_copy(k, 2 * a2 + 1 - b, c).wait_recv()
            loop(0, na, take)

    def rs_done(k):
        for c in range(C):
            def sent(a2):
                s1_copy(k, a2, c).wait_send()
            loop(0, na, sent)

            def sent2(d):
                s2_copy(k, near(d), a, c).wait_send()
                if far:
                    s3_copy(k, near(d), a, c).wait_send()
            loop(1, half, sent2)
            if far:
                s2_copy(k, mirror, a, c).wait_send()

    def ag_done(k):
        for c in range(C):
            def sent(d):
                z_copy(k, fs, near(d), c).wait_send()
                if far:
                    zz_copy(k, near(d), c).wait_send()
            loop(1, half, sent)
            if far:
                z_copy(k, fs, mirror, c).wait_send()

            def sent2(a2):
                y_copy(k, 2 * a2 + b, c).wait_send()
            loop(0, na, sent2)

    for load in loads:
        load.start()
    barrier = pltpu.get_barrier_semaphore()

    def greet(s):
        pl.semaphore_signal(barrier, inc=1, device_id=dev(gr, lax.rem(fs + s, n), tp), device_id_type=MESH)
    loop(1, n, greet)
    for t in others_t:
        pl.semaphore_signal(barrier, inc=1, device_id=dev(gr, fs, t), device_id_type=MESH)
    for g in others_g:
        pl.semaphore_signal(barrier, inc=1, device_id=dev(g, fs, tp), device_id_type=MESH)
    loads[0].wait()
    cast_w(0, 0)
    pl.semaphore_wait(barrier, n + T + G - 3)

    def norm_rows(j):
        p[0, j] = normed_of(prompt[j].astype(f32))

    def start_tokens():
        loads[7].wait()
        loop(0, n, norm_rows)
        flatten(p.at[0])
        st[...] = prompt[fs].astype(f32)

    def unpack(k):
        flatten(ag.at[k])

    def done(k):
        gather_done(k)
        rs_done(k)
        ag_done(k)

    xsend_w(0, 0)
    plane_own(0, 0)
    cast_w(0, 1)
    xsend_w(0, 1)
    plane_own(0, 1)
    cast_d(0)
    xsend_d(0)
    cast_w(1, 0)
    cast_w(1, 1)
    cast_d(1)
    start_tokens()
    xsend_w(1, 0)
    plane_x(0, 0)
    plane_x(0, 1)
    arrive(0, 0)
    arrive(0, 1)
    relay_d(0)
    cross(0, 0)
    landed(0, 0)
    xsend_w(1, 1)
    plane_own(1, 0)
    plane_x(1, 0)
    gates(0)
    cross(0, 1)
    landed(0, 1)
    plane_own(1, 1)
    landed_d(0)
    compute(0)
    rs_first(0)
    plane_x(1, 1)
    xsend_d(1)
    rs_far(0, 0)
    if C > 1:
        rs_far(0, 1)
    arrive(1, 0)
    rs_mid(0, 0)
    if C > 1:
        rs_mid(0, 1)
    rs_near(0, 0)
    if C > 1:
        rs_near(0, 1)
    rs_own(0, 0)
    if C > 1:
        rs_last(0, 0)
        rs_own(0, 1)
    arrive(1, 1)
    rs_last(0, C - 1)
    relay_d(1)
    ag_pass(0, 0)
    if C > 1:
        ag_pass(0, 1)
    ag_far(0, 0)
    if C > 1:
        ag_far(0, 1)
    cross(1, 0)
    ag_take(0)
    unpack(0)
    landed(1, 0)
    gates(1)
    cross(1, 1)
    landed(1, 1)
    landed_d(1)
    compute(1)
    rs_first(1)
    rs_far(1, 0)
    if C > 1:
        rs_far(1, 1)
    rs_mid(1, 0)
    if C > 1:
        rs_mid(1, 1)
    rs_near(1, 0)
    if C > 1:
        rs_near(1, 1)
    rs_own(1, 0)
    if C > 1:
        rs_last(1, 0)
        rs_own(1, 1)
    rs_last(1, C - 1)
    ag_pass(1, 0)
    if C > 1:
        ag_pass(1, 1)
    ag_far(1, 0)
    if C > 1:
        ag_far(1, 1)
    ag_take(1)
    done(0)
    done(1)


def write_out(wall, dn, ag, gate_o, up_o, down_o, mixed_o, o_s, d_s, m_s):
    L, S, _, DC = dn.shape
    copies = []
    for k in range(L):
        copies.append(pltpu.make_async_copy(wall.at[k, 0], gate_o.at[k], o_s.at[k, 0]))
        copies.append(pltpu.make_async_copy(wall.at[k, 1], up_o.at[k], o_s.at[k, 1]))
        for s in range(S):
            copies.append(pltpu.make_async_copy(
                dn.at[k, s], down_o.at[k, :, pl.ds(s * DC, DC)], d_s.at[k, s]))
    copies.append(pltpu.make_async_copy(ag.at[L - 1], mixed_o, m_s))
    for c in copies:
        c.start()
    for c in copies:
        c.wait()


def per_device(G, n, T, prompt, norm_gain, gate_weight, up_weight, down_weight):
    D = prompt.shape[2]
    rows = prompt.shape[0] * prompt.shape[1]
    L, R, C_ = gate_weight.shape
    FFb, DC = down_weight.shape[1:]
    q = C_ // FFb
    tb = rows // n
    na = n // 2
    C = max(1, min(2, tb // 8))
    dma = pltpu.SemaphoreType.DMA
    vmem = pl.BlockSpec(memory_space=pltpu.VMEM)
    anym = pl.BlockSpec(memory_space=pl.ANY)
    wall, dn, ag = pl.pallas_call(
        functools.partial(kernel, G, n, T),
        out_shape=(
            pltpu.VMEM((L, 2, n, R, FFb), bf16),
            pltpu.VMEM((L, G * T, FFb, DC), bf16),
            pltpu.VMEM((L, n, tb, D), bf16),
        ),
        in_specs=[pl.BlockSpec(memory_space=pltpu.HBM)] * 5,
        out_specs=(vmem,) * 3,
        scratch_shapes=[
            pltpu.VMEM((n, tb, D), bf16), pltpu.VMEM((L, R), f32),
            pltpu.VMEM((L, R, C_), f32), pltpu.VMEM((L, R, C_), f32), pltpu.VMEM((L, FFb, DC), f32),
            dma((8,)),
            pltpu.VMEM((L, 2, G, q, R, FFb), bf16),
            pltpu.VMEM((L, n, tb, D), bf16),
            pltpu.VMEM((L, na, tb, D), bf16),
            pltpu.VMEM((L, na, tb, D), bf16),
            pltpu.VMEM((L, na, tb, D), bf16),
            pltpu.VMEM((L, na, tb, D), bf16),
            pltpu.VMEM((tb, D), f32),
            pltpu.VMEM((rows, D), bf16),
            pltpu.VMEM((rows, FFb), bf16),
            pltpu.VMEM((rows, FFb), f32),
            pltpu.VMEM((tb, D), f32),
            dma((L, 2, q, G)), dma((L, 2, q, G)), dma((L, 2, n)), dma((L, 2, 2, n)), dma((L, G)),
            dma((L, 2, G, q)), dma((L, 2, n)), dma((L, 2)), dma((L, 2, 2, n, T)),
            dma((L, G, T)), dma((L, G * T)),
            dma((L, na, C)), dma((L, na, C)), dma((L, na, C)), dma((L, na, C)), dma((L, na, C)), dma((L, na, C)),
            dma((L, na, C)), dma((L, na, C)), dma((L, n, C)), dma((L, na, C)),
        ],
        compiler_params=pltpu.CompilerParams(
            collective_id=0, has_side_effects=True, vmem_limit_bytes=40 * 1024 * 1024),
    )(prompt.reshape(n, tb, D), norm_gain, gate_weight, up_weight, down_weight)
    gate, up, down, mixed = pl.pallas_call(
        write_out,
        out_shape=(
            jax.ShapeDtypeStruct((L, n, R, FFb), bf16),
            jax.ShapeDtypeStruct((L, n, R, FFb), bf16),
            jax.ShapeDtypeStruct((L, FFb, D), bf16),
            jax.ShapeDtypeStruct((n, tb, D), bf16),
        ),
        in_specs=[anym] * 3,
        out_specs=(anym,) * 4,
        scratch_shapes=[dma((L, 2)), dma((L, G * T)), dma(())],
        compiler_params=pltpu.CompilerParams(vmem_limit_bytes=1024 * 1024),
    )(*(pltpu.with_memory_space_constraint(x, pltpu.VMEM) for x in (wall, dn, ag)))
    return (gate.reshape(L, n * R, FFb), up.reshape(L, n * R, FFb), down, mixed.reshape(prompt.shape))


def solution(mesh):
    G, n, T = mesh.shape["gr"], mesh.shape["fs"], mesh.shape["tp"]
    in_specs = (
        P(("gr", "tp"), None, None),
        P(None, "fs"),
        P(None, "fs", ("gr", "tp")),
        P(None, "fs", ("gr", "tp")),
        P(None, "fs", ("gr", "tp")),
    )
    out_specs = (
        P(None, None, "fs"),
        P(None, None, "fs"),
        P(None, "fs", None),
        P(("gr", "tp"), None, None),
    )
    return jax.shard_map(
        functools.partial(per_device, G, n, T),
        mesh=mesh, in_specs=in_specs, out_specs=out_specs, check_vma=False)
```

```python
import functools

import jax
import jax.numpy as jnp
from jax import lax
from jax.experimental import pallas as pl
from jax.experimental.pallas import tpu as pltpu
from jax.sharding import PartitionSpec as P

norm_eps = 1e-06
MESH = pl.DeviceIdType.MESH
f32 = jnp.float32
bf16 = jnp.bfloat16


def kernel(G, n, T, prompt_h, gain_h, gate_h, up_h, down_h,
           wall, dn, ag,
           prompt, gain, gate_w, up_w, down_w, in_s, wsrc, p, r1, q2, r2, r3, sums, hid, gact, st,
           x_s, x_r, v_s, v_r, xd_s, p_s, w_r, w_l, f_s, d_s, d_r,
           s1_s, s1_r, s2_s, s2_r, s3_s, s3_r, g_s, gg_s, g_r, h_s):
    gr, fs, tp = lax.axis_index("gr"), lax.axis_index("fs"), lax.axis_index("tp")
    q, R, FFb = wsrc.shape[3:]
    tb, D = prompt.shape[1:]
    rows = n * tb
    DC = dn.shape[3]
    na = n // 2
    wing = n // 2 if n % 2 == 0 else n
    a, b = fs // 2, lax.rem(fs, 2)
    C = s1_s.shape[2]
    tc = tb // C
    peer = fs + 1 - 2 * b
    is_recv = lax.rem(fs // q, T) == tp
    slot_me = gr * T + tp
    hs = [(R * c // 16) // 16 * 16 if G == 2 else 0 for c in (4, 8)]

    def mine(k, g):
        return pl.ds(pl.multiple_of(g * hs[k], 16), R - hs[k]) if hs[k] else pl.ds(0, R)

    def only(k, g):
        return pl.ds(pl.multiple_of(g * (R - hs[k]), 16), hs[k])

    def dev(g, f, t):
        return {"gr": g, "fs": f, "tp": t}

    def rc(src, dst, ss, rs, d):
        return pltpu.make_async_remote_copy(
            src_ref=src, dst_ref=dst, send_sem=ss, recv_sem=rs,
            device_id=d, device_id_type=MESH)

    def loop(lo, hi, body):
        def step(i, c):
            body(i)
            return c
        lax.fori_loop(lo, hi, step, 0)

    turn = [lax.rem(i + b + 1, q) for i in range(q)]
    others_g = [lax.rem(gr + d, G) for d in range(1, G)]
    loads = [pltpu.make_async_copy(gain_h, gain, in_s.at[0])]
    for k in range(2):
        for h, v in ((gate_h, gate_w), (up_h, up_w), (down_h, down_w)):
            loads.append(pltpu.make_async_copy(h.at[k], v.at[k], in_s.at[len(loads)]))
    loads.append(pltpu.make_async_copy(prompt_h, prompt, in_s.at[len(loads)]))
    others_t = [lax.rem(tp + d, T) for d in range(1, T)]

    def x_copy(k, w, i, g_src, g_dst):
        blk = wsrc.at[k, w, g_src, i, mine(k, g_dst)]
        return rc(blk, blk, x_s.at[k, w, i, g_dst], x_r.at[k, w, i, g_src], dev(g_dst, fs, tp))

    def xd_copy(k, g_src, g_dst):
        blk = dn.at[k, g_src * T + tp]
        return rc(blk, blk, xd_s.at[k, g_dst], d_r.at[k, g_src * T + tp], dev(g_dst, fs, tp))

    def d_copy(k, g_src, t_src, t_dst):
        blk = dn.at[k, g_src * T + t_src]
        return rc(blk, blk, d_s.at[k, g_src, t_dst], d_r.at[k, g_src * T + t_src], dev(gr, fs, t_dst))

    def col_of(g, i):
        return (g * T + tp) * q + i

    def p_copy(k, w, g, i):
        return rc(wsrc.at[k, w, g, i, mine(k, gr)], wall.at[k, w, fs, mine(k, gr)], p_s.at[k, w, g, i],
                  w_r.at[k, w, fs], dev(gr, col_of(g, i), tp))

    def l_copy(k, w, g, i):
        return pltpu.make_async_copy(wsrc.at[k, w, g, i, mine(k, gr)], wall.at[k, w, fs, mine(k, gr)], w_l.at[k, w])

    def f_copy(k, w, f, t):
        blk = wall.at[k, w, f, mine(k, gr)]
        return rc(blk, blk, f_s.at[k, w, 0, f, t], w_r.at[k, w, f], dev(gr, fs, t))

    def v_copy(k, w, f, g_src):
        blk = wall.at[k, w, f, only(k, g_src)]
        return rc(blk, blk, v_s.at[k, w, f], v_r.at[k, w, 0, f], dev(1 - g_src, fs, tp))

    def fv_copy(k, w, f, t):
        blk = wall.at[k, w, f, only(k, 1 - gr)]
        return rc(blk, blk, f_s.at[k, w, 1, f, t], v_r.at[k, w, 1, f], dev(gr, fs, t))

    def column(k):
        eye = lax.broadcasted_iota(jnp.int32, (R, R), 0) == lax.broadcasted_iota(jnp.int32, (R, R), 1)
        return jnp.sum(jnp.where(eye, gain[k:k + 1], 0.0), axis=1, keepdims=True)

    def cast_w(k, w):
        ref = (gate_w, up_w)[w]
        loads[1 + 3 * k + w].wait()
        for i in range(q):
            wsrc[k, w, gr, i] = (column(k) * ref[k, :, i * FFb:(i + 1) * FFb]).astype(bf16)

    def xsend_w(k, w):
        for i in turn:
            for g in others_g:
                x_copy(k, w, i, gr, g).start()

    def cast_d(k):
        loads[3 + 3 * k].wait()
        dn[k, slot_me] = down_w[k].astype(bf16)

    def xsend_d(k):
        for g in others_g:
            xd_copy(k, gr, g).start()
        for t in others_t:
            d_copy(k, gr, tp, t).start()

    def plane(k, w, g, i):
        c = col_of(g, i)

        @pl.when(c != fs)
        def _():
            p_copy(k, w, g, i).start()

        @pl.when(c == fs)
        def _():
            l_copy(k, w, g, i).start()

    def plane_own(k, w):
        for i in turn:
            plane(k, w, gr, i)

    def plane_x(k, w):
        for g in others_g:
            for i in turn:
                x_copy(k, w, i, g, gr).wait_recv()
                plane(k, w, g, i)

    def source(s):
        e = s // wing
        return lax.rem((fs // wing + e) * wing + lax.rem(fs + s, wing), n)

    def arrive(k, w):
        def forward(f):
            for t in others_t:
                f_copy(k, w, f, t).start()
            if hs[k]:
                v_copy(k, w, f, gr).start()

        @pl.when(is_recv)
        def _():
            l_copy(k, w, 0, 0).wait()
            forward(fs)

            def take(s):
                f = source(s)
                f_copy(k, w, f, tp).wait_recv()
                forward(f)
            loop(1, n, take)

    def cross(k, w):
        if hs[k]:
            @pl.when(is_recv)
            def _():
                def take(s):
                    f = source(s)
                    v_copy(k, w, f, 1 - gr).wait_recv()
                    for t in others_t:
                        fv_copy(k, w, f, t).start()
                loop(0, n, take)

    def landed(k, w):
        @pl.when(jnp.logical_not(is_recv))
        def _():
            def take(f):
                f_copy(k, w, f, tp).wait_recv()
                if hs[k]:
                    fv_copy(k, w, f, tp).wait_recv()
            loop(0, n, take)

    def relay_d(k):
        for g in others_g:
            xd_copy(k, g, gr).wait_recv()
            for t in others_t:
                d_copy(k, g, tp, t).start()

    def landed_d(k):
        for g in range(G):
            for t in others_t:
                d_copy(k, g, t, tp).wait_recv()

    def gather_done(k):
        for w in range(2):
            for i in range(q):
                for g in others_g:
                    x_copy(k, w, i, gr, g).wait_send()
            for g in range(G):
                for i in range(q):
                    @pl.when(col_of(g, i) != fs)
                    def _():
                        p_copy(k, w, g, i).wait_send()

            @pl.when(is_recv)
            def _():
                def sent(f):
                    for t in others_t:
                        f_copy(k, w, f, t).wait_send()
                        if hs[k]:
                            fv_copy(k, w, f, t).wait_send()
                    if hs[k]:
                        v_copy(k, w, f, gr).wait_send()
                loop(0, n, sent)
        for g in others_g:
            xd_copy(k, gr, g).wait_send()
        for g in range(G):
            for t in others_t:
                d_copy(k, g, tp, t).wait_send()

    def tokens(k):
        return (p if k == 0 else ag)[0].reshape(rows, D)

    def normed_of(x):
        return (x * lax.rsqrt(jnp.mean(x * x, axis=-1, keepdims=True) + norm_eps)).astype(bf16)

    def gates(k):
        ft = min(FFb, 256)

        def act(j):
            cols = pl.ds(j * ft, ft)
            gact[:, cols] = jnp.dot(tokens(k), wall[k, 0, :, :, cols].reshape(D, ft), preferred_element_type=f32)
        for j in range(FFb // ft):
            act(j)

    def compute(k):
        ft = min(FFb, 256)

        def act(j):
            cols = pl.ds(j * ft, ft)
            gate = gact[:, cols]
            up = jnp.dot(tokens(k), wall[k, 1, :, :, cols].reshape(D, ft), preferred_element_type=f32)
            hid[:, cols] = (gate / (1.0 + jnp.exp(-gate)) * up).astype(bf16)
        for j in range(FFb // ft):
            act(j)

        def proj(s):
            cols = pl.ds(s * DC, DC)
            v = jnp.dot(hid[...], dn[k, s], preferred_element_type=f32)
            p[k, :, :, cols] = v.reshape(n, tb, DC).astype(bf16)
        for s in range(G * T):
            proj(s)

    half = na // 2 if na % 2 == 0 else na
    far = na // half - 1
    pos = lax.rem(a, half)
    mirror = lax.rem(a + half, na)

    def near(d):
        return a - pos + lax.rem(pos + d, half)

    def across(a2):
        return lax.rem(a2 + half, na)

    def part(c):
        return pl.ds(c * tc, tc)

    def s1_copy(k, a2, c):
        return rc(p.at[k, 2 * a2 + 1 - b, part(c)], r1.at[k, a2, part(c)],
                  s1_s.at[k, a2, c], s1_r.at[k, a2, c], dev(gr, peer, tp))

    def s2_copy(k, a2, a_from, c):
        return rc(q2.at[k, a2, part(c)], r2.at[k, a_from, part(c)],
                  s2_s.at[k, a2, c], s2_r.at[k, a_from, c], dev(gr, 2 * a2 + b, tp))

    def s3_copy(k, o, a_from, c):
        return rc(q2.at[k, across(o), part(c)], r3.at[k, a_from, part(c)],
                  s3_s.at[k, o, c], s3_r.at[k, a_from, c], dev(gr, 2 * o + b, tp))

    def rs_first(k):
        def send(of):
            def chunks(d):
                for c in range(C):
                    s1_copy(k, of(d), c).start()
            return chunks
        if far:
            loop(1, half, send(lambda d: across(near(d))))
            send(lambda d: mirror)(0)
        loop(1, half, send(near))
        send(lambda d: a)(0)

    def pair(k, a2, c):
        s1_copy(k, a2, c).wait_recv()
        return p[k, 2 * a2 + b, part(c)].astype(f32) + r1[k, a2, part(c)].astype(f32)

    def rs_far(k, c):
        if far:
            def send(d):
                o = near(d)
                q2[k, across(o), part(c)] = pair(k, across(o), c).astype(bf16)
                s3_copy(k, o, a, c).start()
            loop(1, half, send)

    def rs_near(k, c):
        def send(d):
            o = near(d)
            q2[k, o, part(c)] = pair(k, o, c).astype(bf16)
            s2_copy(k, o, a, c).start()
        loop(1, half, send)

    def rs_mid(k, c):
        if far:
            sums[part(c)] = pair(k, mirror, c)

            def take(d):
                o = near(d)
                s3_copy(k, a, o, c).wait_recv()
                sums[part(c)] += r3[k, o, part(c)].astype(f32)
            loop(1, half, take)
            q2[k, mirror, part(c)] = sums[part(c)].astype(bf16)
            s2_copy(k, mirror, a, c).start()

    def rs_own(k, c):
        st[part(c)] += 0.5 * pair(k, a, c)

    def rs_last(k, c):
        def take(a2):
            s2_copy(k, a2, a2, c).wait_recv()
            st[part(c)] += 0.5 * r2[k, a2, part(c)].astype(f32)
        loop(1, half, lambda d: take(near(d)))
        if far:
            take(mirror)
        x = st[part(c)]
        ag[k, fs, part(c)] = normed_of(x) if k == 0 else x.astype(bf16)

        if far:
            z_copy(k, fs, mirror, c).start()

        def send(d):
            z_copy(k, fs, near(d), c).start()
        loop(1, half, send)
        y_copy(k, fs, c).start()

    def z_copy(k, j, a2, c):
        blk = ag.at[k, j, part(c)]
        return rc(blk, blk, g_s.at[k, a2, c], g_r.at[k, j, c], dev(gr, 2 * a2 + b, tp))

    def y_copy(k, j, c):
        blk = ag.at[k, j, part(c)]
        return rc(blk, blk, h_s.at[k, j // 2, c], g_r.at[k, j, c], dev(gr, peer, tp))

    def zz_copy(k, a2, c):
        blk = ag.at[k, 2 * mirror + b, part(c)]
        return rc(blk, blk, gg_s.at[k, a2, c], g_r.at[k, 2 * mirror + b, c], dev(gr, 2 * a2 + b, tp))

    def pass_on(k, a2, c):
        z_copy(k, 2 * a2 + b, a2, c).wait_recv()
        y_copy(k, 2 * a2 + b, c).start()

    def ag_pass(k, c):
        def own(d):
            pass_on(k, near(d), c)
        loop(1, half, own)
        if far:
            z_copy(k, 2 * mirror + b, a, c).wait_recv()

            def spread(d):
                zz_copy(k, near(d), c).start()
            loop(1, half, spread)
            y_copy(k, 2 * mirror + b, c).start()

    def ag_far(k, c):
        if far:
            def theirs(d):
                pass_on(k, across(near(d)), c)
            loop(1, half, theirs)

    def ag_take(k):
        for c in range(C):
            def take(a2):
                y_copy(k, 2 * a2 + 1 - b, c).wait_recv()
            loop(0, na, take)

    def rs_done(k):
        for c in range(C):
            def sent(a2):
                s1_copy(k, a2, c).wait_send()
            loop(0, na, sent)

            def sent2(d):
                s2_copy(k, near(d), a, c).wait_send()
                if far:
                    s3_copy(k, near(d), a, c).wait_send()
            loop(1, half, sent2)
            if far:
                s2_copy(k, mirror, a, c).wait_send()

    def ag_done(k):
        for c in range(C):
            def sent(d):
                z_copy(k, fs, near(d), c).wait_send()
                if far:
                    zz_copy(k, near(d), c).wait_send()
            loop(1, half, sent)
            if far:
                z_copy(k, fs, mirror, c).wait_send()

            def sent2(a2):
                y_copy(k, 2 * a2 + b, c).wait_send()
            loop(0, na, sent2)

    for load in loads:
        load.start()
    barrier = pltpu.get_barrier_semaphore()

    def greet(s):
        pl.semaphore_signal(barrier, inc=1, device_id=dev(gr, lax.rem(fs + s, n), tp), device_id_type=MESH)
    loop(1, n, greet)
    for t in others_t:
        pl.semaphore_signal(barrier, inc=1, device_id=dev(gr, fs, t), device_id_type=MESH)
    for g in others_g:
        pl.semaphore_signal(barrier, inc=1, device_id=dev(g, fs, tp), device_id_type=MESH)
    loads[0].wait()
    cast_w(0, 0)
    pl.semaphore_wait(barrier, n + T + G - 3)

    def norm_rows(j):
        p[0, j] = normed_of(prompt[j].astype(f32))

    def start_tokens():
        loads[7].wait()
        loop(0, n, norm_rows)
        st[...] = prompt[fs].astype(f32)

    def done(k):
        gather_done(k)
        rs_done(k)
        ag_done(k)

    xsend_w(0, 0)
    plane_own(0, 0)
    cast_w(0, 1)
    xsend_w(0, 1)
    plane_own(0, 1)
    cast_d(0)
    xsend_d(0)
    cast_w(1, 0)
    cast_w(1, 1)
    cast_d(1)
    start_tokens()
    xsend_w(1, 0)
    plane_x(0, 0)
    plane_x(0, 1)
    arrive(0, 0)
    arrive(0, 1)
    relay_d(0)
    cross(0, 0)
    landed(0, 0)
    xsend_w(1, 1)
    plane_own(1, 0)
    plane_x(1, 0)
    gates(0)
    cross(0, 1)
    landed(0, 1)
    plane_own(1, 1)
    landed_d(0)
    compute(0)
    rs_first(0)
    plane_x(1, 1)
    xsend_d(1)
    rs_far(0, 0)
    if C > 1:
        rs_far(0, 1)
    arrive(1, 0)
    rs_mid(0, 0)
    if C > 1:
        rs_mid(0, 1)
    rs_near(0, 0)
    if C > 1:
        rs_near(0, 1)
    rs_own(0, 0)
    if C > 1:
        rs_last(0, 0)
        rs_own(0, 1)
    arrive(1, 1)
    rs_last(0, C - 1)
    relay_d(1)
    ag_pass(0, 0)
    if C > 1:
        ag_pass(0, 1)
    ag_far(0, 0)
    if C > 1:
        ag_far(0, 1)
    cross(1, 0)
    ag_take(0)
    landed(1, 0)
    gates(1)
    cross(1, 1)
    landed(1, 1)
    landed_d(1)
    compute(1)
    rs_first(1)
    done(0)
    rs_far(1, 0)
    if C > 1:
        rs_far(1, 1)
    rs_mid(1, 0)
    if C > 1:
        rs_mid(1, 1)
    rs_near(1, 0)
    if C > 1:
        rs_near(1, 1)
    rs_own(1, 0)
    if C > 1:
        rs_last(1, 0)
        rs_own(1, 1)
    rs_last(1, C - 1)
    ag_pass(1, 0)
    if C > 1:
        ag_pass(1, 1)
    ag_far(1, 0)
    if C > 1:
        ag_far(1, 1)
    gather_done(1)
    rs_done(1)
    ag_take(1)
    ag_done(1)


def write_out(wall, dn, ag, gate_o, up_o, down_o, mixed_o, o_s, d_s, m_s):
    L, S, _, DC = dn.shape
    copies = []
    for k in range(L):
        copies.append(pltpu.make_async_copy(wall.at[k, 0], gate_o.at[k], o_s.at[k, 0]))
        copies.append(pltpu.make_async_copy(wall.at[k, 1], up_o.at[k], o_s.at[k, 1]))
        for s in range(S):
            copies.append(pltpu.make_async_copy(
                dn.at[k, s], down_o.at[k, :, pl.ds(s * DC, DC)], d_s.at[k, s]))
    copies.append(pltpu.make_async_copy(ag.at[L - 1], mixed_o, m_s))
    for c in copies:
        c.start()
    for c in copies:
        c.wait()


def per_device(G, n, T, prompt, norm_gain, gate_weight, up_weight, down_weight):
    D = prompt.shape[2]
    rows = prompt.shape[0] * prompt.shape[1]
    L, R, C_ = gate_weight.shape
    FFb, DC = down_weight.shape[1:]
    q = C_ // FFb
    tb = rows // n
    na = n // 2
    C = max(1, min(2, tb // 8))
    dma = pltpu.SemaphoreType.DMA
    vmem = pl.BlockSpec(memory_space=pltpu.VMEM)
    anym = pl.BlockSpec(memory_space=pl.ANY)
    wall, dn, ag = pl.pallas_call(
        functools.partial(kernel, G, n, T),
        out_shape=(
            pltpu.VMEM((L, 2, n, R, FFb), bf16),
            pltpu.VMEM((L, G * T, FFb, DC), bf16),
            pltpu.VMEM((L, n, tb, D), bf16),
        ),
        in_specs=[pl.BlockSpec(memory_space=pltpu.HBM)] * 5,
        out_specs=(vmem,) * 3,
        scratch_shapes=[
            pltpu.VMEM((n, tb, D), bf16), pltpu.VMEM((L, R), f32),
            pltpu.VMEM((L, R, C_), f32), pltpu.VMEM((L, R, C_), f32), pltpu.VMEM((L, FFb, DC), f32),
            dma((8,)),
            pltpu.VMEM((L, 2, G, q, R, FFb), bf16),
            pltpu.VMEM((L, n, tb, D), bf16),
            pltpu.VMEM((L, na, tb, D), bf16),
            pltpu.VMEM((L, na, tb, D), bf16),
            pltpu.VMEM((L, na, tb, D), bf16),
            pltpu.VMEM((L, na, tb, D), bf16),
            pltpu.VMEM((tb, D), f32),
            pltpu.VMEM((rows, FFb), bf16),
            pltpu.VMEM((rows, FFb), f32),
            pltpu.VMEM((tb, D), f32),
            dma((L, 2, q, G)), dma((L, 2, q, G)), dma((L, 2, n)), dma((L, 2, 2, n)), dma((L, G)),
            dma((L, 2, G, q)), dma((L, 2, n)), dma((L, 2)), dma((L, 2, 2, n, T)),
            dma((L, G, T)), dma((L, G * T)),
            dma((L, na, C)), dma((L, na, C)), dma((L, na, C)), dma((L, na, C)), dma((L, na, C)), dma((L, na, C)),
            dma((L, na, C)), dma((L, na, C)), dma((L, n, C)), dma((L, na, C)),
        ],
        compiler_params=pltpu.CompilerParams(
            collective_id=0, has_side_effects=True, vmem_limit_bytes=40 * 1024 * 1024),
    )(prompt.reshape(n, tb, D), norm_gain, gate_weight, up_weight, down_weight)
    gate, up, down, mixed = pl.pallas_call(
        write_out,
        out_shape=(
            jax.ShapeDtypeStruct((L, n, R, FFb), bf16),
            jax.ShapeDtypeStruct((L, n, R, FFb), bf16),
            jax.ShapeDtypeStruct((L, FFb, D), bf16),
            jax.ShapeDtypeStruct((n, tb, D), bf16),
        ),
        in_specs=[anym] * 3,
        out_specs=(anym,) * 4,
        scratch_shapes=[dma((L, 2)), dma((L, G * T)), dma(())],
        compiler_params=pltpu.CompilerParams(vmem_limit_bytes=1024 * 1024),
    )(*(pltpu.with_memory_space_constraint(x, pltpu.VMEM) for x in (wall, dn, ag)))
    return (gate.reshape(L, n * R, FFb), up.reshape(L, n * R, FFb), down, mixed.reshape(prompt.shape))


def solution(mesh):
    G, n, T = mesh.shape["gr"], mesh.shape["fs"], mesh.shape["tp"]
    in_specs = (
        P(("gr", "tp"), None, None),
        P(None, "fs"),
        P(None, "fs", ("gr", "tp")),
        P(None, "fs", ("gr", "tp")),
        P(None, "fs", ("gr", "tp")),
    )
    out_specs = (
        P(None, None, "fs"),
        P(None, None, "fs"),
        P(None, "fs", None),
        P(("gr", "tp"), None, None),
    )
    return jax.shard_map(
        functools.partial(per_device, G, n, T),
        mesh=mesh, in_specs=in_specs, out_specs=out_specs, check_vma=False)
```

```python
import functools

import jax
import jax.numpy as jnp
from jax import lax
from jax.experimental import pallas as pl
from jax.experimental.pallas import tpu as pltpu
from jax.sharding import PartitionSpec as P

norm_eps = 1e-06
MESH = pl.DeviceIdType.MESH
f32 = jnp.float32
bf16 = jnp.bfloat16


def kernel(G, n, T, prompt_h, gain_h, gate_h, up_h, down_h,
           wall, dn, ag,
           prompt, gain, gate_w, up_w, down_w, in_s, wsrc, p, r1, q2, r2, r3, sums, hid, gact, st,
           x_s, x_r, v_s, v_r, xd_s, p_s, w_r, w_l, f_s, d_s, d_r,
           s1_s, s1_r, s2_s, s2_r, s3_s, s3_r, g_s, gg_s, g_r, h_s):
    gr, fs, tp = lax.axis_index("gr"), lax.axis_index("fs"), lax.axis_index("tp")
    q, R, FFb = wsrc.shape[3:]
    tb, D = prompt.shape[1:]
    rows = n * tb
    DC = dn.shape[3]
    na = n // 2
    wing = n // 2 if n % 2 == 0 else n
    a, b = fs // 2, lax.rem(fs, 2)
    C = s1_s.shape[2]
    tc = tb // C
    peer = fs + 1 - 2 * b
    is_recv = lax.rem(fs // q, T) == tp
    slot_me = gr * T + tp
    hs = [(R * c // 16) // 16 * 16 if G == 2 else 0 for c in (4, 8)]

    def mine(k, g):
        return pl.ds(pl.multiple_of(g * hs[k], 16), R - hs[k]) if hs[k] else pl.ds(0, R)

    def only(k, g):
        return pl.ds(pl.multiple_of(g * (R - hs[k]), 16), hs[k])

    def dev(g, f, t):
        return {"gr": g, "fs": f, "tp": t}

    def rc(src, dst, ss, rs, d):
        return pltpu.make_async_remote_copy(
            src_ref=src, dst_ref=dst, send_sem=ss, recv_sem=rs,
            device_id=d, device_id_type=MESH)

    def loop(lo, hi, body):
        def step(i, c):
            body(i)
            return c
        lax.fori_loop(lo, hi, step, 0)

    turn = [lax.rem(i + b + 1, q) for i in range(q)]
    others_g = [lax.rem(gr + d, G) for d in range(1, G)]
    loads = [pltpu.make_async_copy(gain_h, gain, in_s.at[0])]
    for k in range(2):
        for h, v in ((gate_h, gate_w), (up_h, up_w), (down_h, down_w)):
            loads.append(pltpu.make_async_copy(h.at[k], v.at[k], in_s.at[len(loads)]))
    loads.append(pltpu.make_async_copy(prompt_h, prompt, in_s.at[len(loads)]))
    others_t = [lax.rem(tp + d, T) for d in range(1, T)]

    def x_copy(k, w, i, g_src, g_dst):
        blk = wsrc.at[k, w, g_src, i, mine(k, g_dst)]
        return rc(blk, blk, x_s.at[k, w, i, g_dst], x_r.at[k, w, i, g_src], dev(g_dst, fs, tp))

    def xd_copy(k, g_src, g_dst):
        blk = dn.at[k, g_src * T + tp]
        return rc(blk, blk, xd_s.at[k, g_dst], d_r.at[k, g_src * T + tp], dev(g_dst, fs, tp))

    def d_copy(k, g_src, t_src, t_dst):
        blk = dn.at[k, g_src * T + t_src]
        return rc(blk, blk, d_s.at[k, g_src, t_dst], d_r.at[k, g_src * T + t_src], dev(gr, fs, t_dst))

    def col_of(g, i):
        return (g * T + tp) * q + i

    def p_copy(k, w, g, i):
        return rc(wsrc.at[k, w, g, i, mine(k, gr)], wall.at[k, w, fs, mine(k, gr)], p_s.at[k, w, g, i],
                  w_r.at[k, w, fs], dev(gr, col_of(g, i), tp))

    def l_copy(k, w, g, i):
        return pltpu.make_async_copy(wsrc.at[k, w, g, i, mine(k, gr)], wall.at[k, w, fs, mine(k, gr)], w_l.at[k, w])

    def f_copy(k, w, f, t):
        blk = wall.at[k, w, f, mine(k, gr)]
        return rc(blk, blk, f_s.at[k, w, 0, f, t], w_r.at[k, w, f], dev(gr, fs, t))

    def v_copy(k, w, f, g_src):
        blk = wall.at[k, w, f, only(k, g_src)]
        return rc(blk, blk, v_s.at[k, w, f], v_r.at[k, w, 0, f], dev(1 - g_src, fs, tp))

    def fv_copy(k, w, f, t):
        blk = wall.at[k, w, f, only(k, 1 - gr)]
        return rc(blk, blk, f_s.at[k, w, 1, f, t], v_r.at[k, w, 1, f], dev(gr, fs, t))

    def column(k):
        eye = lax.broadcasted_iota(jnp.int32, (R, R), 0) == lax.broadcasted_iota(jnp.int32, (R, R), 1)
        return jnp.sum(jnp.where(eye, gain[k:k + 1], 0.0), axis=1, keepdims=True)

    def cast_w(k, w):
        ref = (gate_w, up_w)[w]
        loads[1 + 3 * k + w].wait()
        for i in range(q):
            wsrc[k, w, gr, i] = (column(k) * ref[k, :, i * FFb:(i + 1) * FFb]).astype(bf16)

    def xsend_w(k, w):
        for i in turn:
            for g in others_g:
                x_copy(k, w, i, gr, g).start()

    def cast_d(k):
        loads[3 + 3 * k].wait()
        dn[k, slot_me] = down_w[k].astype(bf16)

    def xsend_d(k):
        for g in others_g:
            xd_copy(k, gr, g).start()
        for t in others_t:
            d_copy(k, gr, tp, t).start()

    def plane(k, w, g, i):
        c = col_of(g, i)

        @pl.when(c != fs)
        def _():
            p_copy(k, w, g, i).start()

        @pl.when(c == fs)
        def _():
            l_copy(k, w, g, i).start()

    def plane_own(k, w):
        for i in turn:
            plane(k, w, gr, i)

    def plane_x(k, w):
        for g in others_g:
            for i in turn:
                x_copy(k, w, i, g, gr).wait_recv()
                plane(k, w, g, i)

    def source(s):
        e = s // wing
        return lax.rem((fs // wing + e) * wing + lax.rem(fs + s, wing), n)

    def arrive(k, w):
        def forward(f):
            for t in others_t:
                f_copy(k, w, f, t).start()
            if hs[k]:
                v_copy(k, w, f, gr).start()

        @pl.when(is_recv)
        def _():
            l_copy(k, w, 0, 0).wait()
            forward(fs)

            def take(s):
                f = source(s)
                f_copy(k, w, f, tp).wait_recv()
                forward(f)
            loop(1, n, take)

    def cross(k, w):
        if hs[k]:
            @pl.when(is_recv)
            def _():
                def take(s):
                    f = source(s)
                    v_copy(k, w, f, 1 - gr).wait_recv()
                    for t in others_t:
                        fv_copy(k, w, f, t).start()
                loop(0, n, take)

    def landed(k, w):
        @pl.when(jnp.logical_not(is_recv))
        def _():
            def take(f):
                f_copy(k, w, f, tp).wait_recv()
                if hs[k]:
                    fv_copy(k, w, f, tp).wait_recv()
            loop(0, n, take)

    def relay_d(k):
        for g in others_g:
            xd_copy(k, g, gr).wait_recv()
            for t in others_t:
                d_copy(k, g, tp, t).start()

    def landed_d(k):
        for g in range(G):
            for t in others_t:
                d_copy(k, g, t, tp).wait_recv()

    def gather_done(k):
        for w in range(2):
            for i in range(q):
                for g in others_g:
                    x_copy(k, w, i, gr, g).wait_send()
            for g in range(G):
                for i in range(q):
                    @pl.when(col_of(g, i) != fs)
                    def _():
                        p_copy(k, w, g, i).wait_send()

            @pl.when(is_recv)
            def _():
                def sent(f):
                    for t in others_t:
                        f_copy(k, w, f, t).wait_send()
                        if hs[k]:
                            fv_copy(k, w, f, t).wait_send()
                    if hs[k]:
                        v_copy(k, w, f, gr).wait_send()
                loop(0, n, sent)
        for g in others_g:
            xd_copy(k, gr, g).wait_send()
        for g in range(G):
            for t in others_t:
                d_copy(k, g, tp, t).wait_send()

    def tokens(k):
        return (p if k == 0 else ag)[0].reshape(rows, D)

    def normed_of(x):
        return (x * lax.rsqrt(jnp.mean(x * x, axis=-1, keepdims=True) + norm_eps)).astype(bf16)

    def gates(k):
        ft = min(FFb, 256)

        def act(j):
            cols = pl.ds(j * ft, ft)
            gact[:, cols] = jnp.dot(tokens(k), wall[k, 0, :, :, cols].reshape(D, ft), preferred_element_type=f32)
        for j in range(FFb // ft):
            act(j)

    def compute(k):
        ft = min(FFb, 256)

        def act(j):
            cols = pl.ds(j * ft, ft)
            gate = gact[:, cols]
            up = jnp.dot(tokens(k), wall[k, 1, :, :, cols].reshape(D, ft), preferred_element_type=f32)
            hid[:, cols] = (gate / (1.0 + jnp.exp(-gate)) * up).astype(bf16)
        for j in range(FFb // ft):
            act(j)

        def proj(s):
            cols = pl.ds(s * DC, DC)
            v = jnp.dot(hid[...], dn[k, s], preferred_element_type=f32)
            p[k, :, :, cols] = v.reshape(n, tb, DC).astype(bf16)
        for s in range(G * T):
            proj(s)

    half = na // 2 if na % 2 == 0 else na
    far = na // half - 1
    pos = lax.rem(a, half)
    mirror = lax.rem(a + half, na)

    def near(d):
        return a - pos + lax.rem(pos + d, half)

    def across(a2):
        return lax.rem(a2 + half, na)

    def part(c):
        return pl.ds(c * tc, tc)

    def s1_copy(k, a2, c):
        return rc(p.at[k, 2 * a2 + 1 - b, part(c)], r1.at[k, a2, part(c)],
                  s1_s.at[k, a2, c], s1_r.at[k, a2, c], dev(gr, peer, tp))

    def s2_copy(k, a2, a_from, c):
        return rc(q2.at[k, a2, part(c)], r2.at[k, a_from, part(c)],
                  s2_s.at[k, a2, c], s2_r.at[k, a_from, c], dev(gr, 2 * a2 + b, tp))

    def s3_copy(k, o, a_from, c):
        return rc(q2.at[k, across(o), part(c)], r3.at[k, a_from, part(c)],
                  s3_s.at[k, o, c], s3_r.at[k, a_from, c], dev(gr, 2 * o + b, tp))

    def rs_first(k):
        def send(of):
            def chunks(d):
                for c in range(C):
                    s1_copy(k, of(d), c).start()
            return chunks
        if far:
            loop(1, half, send(lambda d: across(near(d))))
            send(lambda d: mirror)(0)
        loop(1, half, send(near))
        send(lambda d: a)(0)

    def pair(k, a2, c):
        s1_copy(k, a2, c).wait_recv()
        return p[k, 2 * a2 + b, part(c)].astype(f32) + r1[k, a2, part(c)].astype(f32)

    def rs_far(k, c):
        if far:
            def send(d):
                o = near(d)
                q2[k, across(o), part(c)] = pair(k, across(o), c).astype(bf16)
                s3_copy(k, o, a, c).start()
            loop(1, half, send)

    def rs_near(k, c):
        def send(d):
            o = near(d)
            q2[k, o, part(c)] = pair(k, o, c).astype(bf16)
            s2_copy(k, o, a, c).start()
        loop(1, half, send)

    def rs_mid(k, c):
        if far:
            sums[part(c)] = pair(k, mirror, c)

            def take(d):
                o = near(d)
                s3_copy(k, a, o, c).wait_recv()
                sums[part(c)] += r3[k, o, part(c)].astype(f32)
            loop(1, half, take)
            q2[k, mirror, part(c)] = sums[part(c)].astype(bf16)
            s2_copy(k, mirror, a, c).start()

    def rs_own(k, c):
        st[part(c)] += 0.5 * pair(k, a, c)

    def rs_last(k, c):
        def take(a2):
            s2_copy(k, a2, a2, c).wait_recv()
            st[part(c)] += 0.5 * r2[k, a2, part(c)].astype(f32)
        loop(1, half, lambda d: take(near(d)))
        if far:
            take(mirror)
        x = st[part(c)]
        ag[k, fs, part(c)] = normed_of(x) if k == 0 else x.astype(bf16)

        if far:
            z_copy(k, fs, mirror, c).start()

        def send(d):
            z_copy(k, fs, near(d), c).start()
        loop(1, half, send)
        y_copy(k, fs, c).start()

    def z_copy(k, j, a2, c):
        blk = ag.at[k, j, part(c)]
        return rc(blk, blk, g_s.at[k, a2, c], g_r.at[k, j, c], dev(gr, 2 * a2 + b, tp))

    def y_copy(k, j, c):
        blk = ag.at[k, j, part(c)]
        return rc(blk, blk, h_s.at[k, j // 2, c], g_r.at[k, j, c], dev(gr, peer, tp))

    def zz_copy(k, a2, c):
        blk = ag.at[k, 2 * mirror + b, part(c)]
        return rc(blk, blk, gg_s.at[k, a2, c], g_r.at[k, 2 * mirror + b, c], dev(gr, 2 * a2 + b, tp))

    def pass_on(k, a2, c):
        z_copy(k, 2 * a2 + b, a2, c).wait_recv()
        y_copy(k, 2 * a2 + b, c).start()

    def ag_pass(k, c):
        def own(d):
            pass_on(k, near(d), c)
        loop(1, half, own)
        if far:
            z_copy(k, 2 * mirror + b, a, c).wait_recv()

            def spread(d):
                zz_copy(k, near(d), c).start()
            loop(1, half, spread)
            y_copy(k, 2 * mirror + b, c).start()

    def ag_far(k, c):
        if far:
            def theirs(d):
                pass_on(k, across(near(d)), c)
            loop(1, half, theirs)

    def ag_take(k):
        for c in range(C):
            def take(a2):
                y_copy(k, 2 * a2 + 1 - b, c).wait_recv()
            loop(0, na, take)

    def rs_done(k):
        for c in range(C):
            def sent(a2):
                s1_copy(k, a2, c).wait_send()
            loop(0, na, sent)

            def sent2(d):
                s2_copy(k, near(d), a, c).wait_send()
                if far:
                    s3_copy(k, near(d), a, c).wait_send()
            loop(1, half, sent2)
            if far:
                s2_copy(k, mirror, a, c).wait_send()

    def ag_done(k):
        for c in range(C):
            def sent(d):
                z_copy(k, fs, near(d), c).wait_send()
                if far:
                    zz_copy(k, near(d), c).wait_send()
            loop(1, half, sent)
            if far:
                z_copy(k, fs, mirror, c).wait_send()

            def sent2(a2):
                y_copy(k, 2 * a2 + b, c).wait_send()
            loop(0, na, sent2)

    for load in loads:
        load.start()
    barrier = pltpu.get_barrier_semaphore()

    def greet(s):
        pl.semaphore_signal(barrier, inc=1, device_id=dev(gr, lax.rem(fs + s, n), tp), device_id_type=MESH)
    loop(1, n, greet)
    for t in others_t:
        pl.semaphore_signal(barrier, inc=1, device_id=dev(gr, fs, t), device_id_type=MESH)
    for g in others_g:
        pl.semaphore_signal(barrier, inc=1, device_id=dev(g, fs, tp), device_id_type=MESH)
    loads[0].wait()
    cast_w(0, 0)
    pl.semaphore_wait(barrier, n + T + G - 3)

    def norm_rows(j):
        p[0, j] = normed_of(prompt[j].astype(f32))

    def start_tokens():
        loads[7].wait()
        loop(0, n, norm_rows)
        st[...] = prompt[fs].astype(f32)

    def done(k):
        gather_done(k)
        rs_done(k)
        ag_done(k)

    xsend_w(0, 0)
    plane_own(0, 0)
    cast_w(0, 1)
    xsend_w(0, 1)
    plane_own(0, 1)
    cast_d(0)
    xsend_d(0)
    cast_w(1, 0)
    cast_w(1, 1)
    cast_d(1)
    start_tokens()
    xsend_w(1, 0)
    plane_x(0, 0)
    plane_x(0, 1)
    arrive(0, 0)
    arrive(0, 1)
    relay_d(0)
    cross(0, 0)
    landed(0, 0)
    xsend_w(1, 1)
    plane_x(1, 0)
    plane_own(1, 0)
    gates(0)
    cross(0, 1)
    landed(0, 1)
    plane_own(1, 1)
    landed_d(0)
    compute(0)
    rs_first(0)
    xsend_d(1)
    plane_x(1, 1)
    rs_far(0, 0)
    if C > 1:
        rs_far(0, 1)
    arrive(1, 0)
    rs_mid(0, 0)
    if C > 1:
        rs_mid(0, 1)
    rs_near(0, 0)
    if C > 1:
        rs_near(0, 1)
    rs_own(0, 0)
    if C > 1:
        rs_last(0, 0)
        rs_own(0, 1)
    arrive(1, 1)
    rs_last(0, C - 1)
    relay_d(1)
    ag_pass(0, 0)
    if C > 1:
        ag_pass(0, 1)
    ag_far(0, 0)
    if C > 1:
        ag_far(0, 1)
    cross(1, 0)
    ag_take(0)
    landed(1, 0)
    gates(1)
    cross(1, 1)
    landed(1, 1)
    landed_d(1)
    compute(1)
    rs_first(1)
    done(0)
    rs_far(1, 0)
    if C > 1:
        rs_far(1, 1)
    rs_mid(1, 0)
    if C > 1:
        rs_mid(1, 1)
    rs_near(1, 0)
    if C > 1:
        rs_near(1, 1)
    rs_own(1, 0)
    if C > 1:
        rs_last(1, 0)
        rs_own(1, 1)
    rs_last(1, C - 1)
    ag_pass(1, 0)
    if C > 1:
        ag_pass(1, 1)
    ag_far(1, 0)
    if C > 1:
        ag_far(1, 1)
    gather_done(1)
    rs_done(1)
    ag_take(1)
    ag_done(1)


def write_out(wall, dn, ag, gate_o, up_o, down_o, mixed_o, o_s, d_s, m_s):
    L, S, _, DC = dn.shape
    copies = []
    for k in range(L):
        copies.append(pltpu.make_async_copy(wall.at[k, 0], gate_o.at[k], o_s.at[k, 0]))
        copies.append(pltpu.make_async_copy(wall.at[k, 1], up_o.at[k], o_s.at[k, 1]))
        for s in range(S):
            copies.append(pltpu.make_async_copy(
                dn.at[k, s], down_o.at[k, :, pl.ds(s * DC, DC)], d_s.at[k, s]))
    copies.append(pltpu.make_async_copy(ag.at[L - 1], mixed_o, m_s))
    for c in copies:
        c.start()
    for c in copies:
        c.wait()


def per_device(G, n, T, prompt, norm_gain, gate_weight, up_weight, down_weight):
    D = prompt.shape[2]
    rows = prompt.shape[0] * prompt.shape[1]
    L, R, C_ = gate_weight.shape
    FFb, DC = down_weight.shape[1:]
    q = C_ // FFb
    tb = rows // n
    na = n // 2
    C = max(1, min(2, tb // 8))
    dma = pltpu.SemaphoreType.DMA
    vmem = pl.BlockSpec(memory_space=pltpu.VMEM)
    anym = pl.BlockSpec(memory_space=pl.ANY)
    wall, dn, ag = pl.pallas_call(
        functools.partial(kernel, G, n, T),
        out_shape=(
            pltpu.VMEM((L, 2, n, R, FFb), bf16),
            pltpu.VMEM((L, G * T, FFb, DC), bf16),
            pltpu.VMEM((L, n, tb, D), bf16),
        ),
        in_specs=[pl.BlockSpec(memory_space=pltpu.HBM)] * 5,
        out_specs=(vmem,) * 3,
        scratch_shapes=[
            pltpu.VMEM((n, tb, D), bf16), pltpu.VMEM((L, R), f32),
            pltpu.VMEM((L, R, C_), f32), pltpu.VMEM((L, R, C_), f32), pltpu.VMEM((L, FFb, DC), f32),
            dma((8,)),
            pltpu.VMEM((L, 2, G, q, R, FFb), bf16),
            pltpu.VMEM((L, n, tb, D), bf16),
            pltpu.VMEM((L, na, tb, D), bf16),
            pltpu.VMEM((L, na, tb, D), bf16),
            pltpu.VMEM((L, na, tb, D), bf16),
            pltpu.VMEM((L, na, tb, D), bf16),
            pltpu.VMEM((tb, D), f32),
            pltpu.VMEM((rows, FFb), bf16),
            pltpu.VMEM((rows, FFb), f32),
            pltpu.VMEM((tb, D), f32),
            dma((L, 2, q, G)), dma((L, 2, q, G)), dma((L, 2, n)), dma((L, 2, 2, n)), dma((L, G)),
            dma((L, 2, G, q)), dma((L, 2, n)), dma((L, 2)), dma((L, 2, 2, n, T)),
            dma((L, G, T)), dma((L, G * T)),
            dma((L, na, C)), dma((L, na, C)), dma((L, na, C)), dma((L, na, C)), dma((L, na, C)), dma((L, na, C)),
            dma((L, na, C)), dma((L, na, C)), dma((L, n, C)), dma((L, na, C)),
        ],
        compiler_params=pltpu.CompilerParams(
            collective_id=0, has_side_effects=True, vmem_limit_bytes=40 * 1024 * 1024),
    )(prompt.reshape(n, tb, D), norm_gain, gate_weight, up_weight, down_weight)
    gate, up, down, mixed = pl.pallas_call(
        write_out,
        out_shape=(
            jax.ShapeDtypeStruct((L, n, R, FFb), bf16),
            jax.ShapeDtypeStruct((L, n, R, FFb), bf16),
            jax.ShapeDtypeStruct((L, FFb, D), bf16),
            jax.ShapeDtypeStruct((n, tb, D), bf16),
        ),
        in_specs=[anym] * 3,
        out_specs=(anym,) * 4,
        scratch_shapes=[dma((L, 2)), dma((L, G * T)), dma(())],
        compiler_params=pltpu.CompilerParams(vmem_limit_bytes=1024 * 1024),
    )(*(pltpu.with_memory_space_constraint(x, pltpu.VMEM) for x in (wall, dn, ag)))
    return (gate.reshape(L, n * R, FFb), up.reshape(L, n * R, FFb), down, mixed.reshape(prompt.shape))


def solution(mesh):
    G, n, T = mesh.shape["gr"], mesh.shape["fs"], mesh.shape["tp"]
    in_specs = (
        P(("gr", "tp"), None, None),
        P(None, "fs"),
        P(None, "fs", ("gr", "tp")),
        P(None, "fs", ("gr", "tp")),
        P(None, "fs", ("gr", "tp")),
    )
    out_specs = (
        P(None, None, "fs"),
        P(None, None, "fs"),
        P(None, "fs", None),
        P(("gr", "tp"), None, None),
    )
    return jax.shard_map(
        functools.partial(per_device, G, n, T),
        mesh=mesh, in_specs=in_specs, out_specs=out_specs, check_vma=False)
```

```python
import functools

import jax
import jax.numpy as jnp
from jax import lax
from jax.experimental import pallas as pl
from jax.experimental.pallas import tpu as pltpu
from jax.sharding import PartitionSpec as P

norm_eps = 1e-06
MESH = pl.DeviceIdType.MESH
f32 = jnp.float32
bf16 = jnp.bfloat16


def kernel(G, n, T, prompt_h, gain_h, gate_h, up_h, down_h,
           wall, dn, ag,
           prompt, gain, gate_w, up_w, down_w, in_s, wsrc, p, r1, q2, r2, r3, sums, hid, gact, st,
           x_s, x_r, v_s, v_r, xd_s, p_s, w_r, w_l, f_s, d_s, d_r,
           s1_s, s1_r, s2_s, s2_r, s3_s, s3_r, g_s, gg_s, g_r, h_s):
    gr, fs, tp = lax.axis_index("gr"), lax.axis_index("fs"), lax.axis_index("tp")
    q, R, FFb = wsrc.shape[3:]
    tb, D = prompt.shape[1:]
    rows = n * tb
    DC = dn.shape[3]
    na = n // 2
    wing = n // 2 if n % 2 == 0 else n
    a, b = fs // 2, lax.rem(fs, 2)
    C = s1_s.shape[2]
    tc = tb // C
    peer = fs + 1 - 2 * b
    is_recv = lax.rem(fs // q, T) == tp
    slot_me = gr * T + tp
    hs = [(R * c // 16) // 16 * 16 if G == 2 else 0 for c in (4, 8)]

    def mine(k, g):
        return pl.ds(pl.multiple_of(g * hs[k], 16), R - hs[k]) if hs[k] else pl.ds(0, R)

    def only(k, g):
        return pl.ds(pl.multiple_of(g * (R - hs[k]), 16), hs[k])

    def dev(g, f, t):
        return {"gr": g, "fs": f, "tp": t}

    def rc(src, dst, ss, rs, d):
        return pltpu.make_async_remote_copy(
            src_ref=src, dst_ref=dst, send_sem=ss, recv_sem=rs,
            device_id=d, device_id_type=MESH)

    def loop(lo, hi, body):
        def step(i, c):
            body(i)
            return c
        lax.fori_loop(lo, hi, step, 0)

    turn = [lax.rem(i + b + 1, q) for i in range(q)]
    others_g = [lax.rem(gr + d, G) for d in range(1, G)]
    loads = [pltpu.make_async_copy(gain_h, gain, in_s.at[0])]
    for k in range(2):
        for h, v in ((gate_h, gate_w), (up_h, up_w), (down_h, down_w)):
            loads.append(pltpu.make_async_copy(h.at[k], v.at[k], in_s.at[len(loads)]))
    loads.append(pltpu.make_async_copy(prompt_h, prompt, in_s.at[len(loads)]))
    others_t = [lax.rem(tp + d, T) for d in range(1, T)]

    def x_copy(k, w, i, g_src, g_dst):
        blk = wsrc.at[k, w, g_src, i, mine(k, g_dst)]
        return rc(blk, blk, x_s.at[k, w, i, g_dst], x_r.at[k, w, i, g_src], dev(g_dst, fs, tp))

    def xd_copy(k, g_src, g_dst):
        blk = dn.at[k, g_src * T + tp]
        return rc(blk, blk, xd_s.at[k, g_dst], d_r.at[k, g_src * T + tp], dev(g_dst, fs, tp))

    def d_copy(k, g_src, t_src, t_dst):
        blk = dn.at[k, g_src * T + t_src]
        return rc(blk, blk, d_s.at[k, g_src, t_dst], d_r.at[k, g_src * T + t_src], dev(gr, fs, t_dst))

    def col_of(g, i):
        return (g * T + tp) * q + i

    def p_copy(k, w, g, i):
        return rc(wsrc.at[k, w, g, i, mine(k, gr)], wall.at[k, w, fs, mine(k, gr)], p_s.at[k, w, g, i],
                  w_r.at[k, w, fs], dev(gr, col_of(g, i), tp))

    def l_copy(k, w, g, i):
        return pltpu.make_async_copy(wsrc.at[k, w, g, i, mine(k, gr)], wall.at[k, w, fs, mine(k, gr)], w_l.at[k, w])

    def f_copy(k, w, f, t):
        blk = wall.at[k, w, f, mine(k, gr)]
        return rc(blk, blk, f_s.at[k, w, 0, f, t], w_r.at[k, w, f], dev(gr, fs, t))

    def v_copy(k, w, f, g_src):
        blk = wall.at[k, w, f, only(k, g_src)]
        return rc(blk, blk, v_s.at[k, w, f], v_r.at[k, w, 0, f], dev(1 - g_src, fs, tp))

    def fv_copy(k, w, f, t):
        blk = wall.at[k, w, f, only(k, 1 - gr)]
        return rc(blk, blk, f_s.at[k, w, 1, f, t], v_r.at[k, w, 1, f], dev(gr, fs, t))

    def column(k):
        eye = lax.broadcasted_iota(jnp.int32, (R, R), 0) == lax.broadcasted_iota(jnp.int32, (R, R), 1)
        return jnp.sum(jnp.where(eye, gain[k:k + 1], 0.0), axis=1, keepdims=True)

    def cast_w(k, w):
        ref = (gate_w, up_w)[w]
        loads[1 + 3 * k + w].wait()
        for i in range(q):
            wsrc[k, w, gr, i] = (column(k) * ref[k, :, i * FFb:(i + 1) * FFb]).astype(bf16)

    def xsend_w(k, w):
        for i in turn:
            for g in others_g:
                x_copy(k, w, i, gr, g).start()

    def cast_d(k):
        loads[3 + 3 * k].wait()
        dn[k, slot_me] = down_w[k].astype(bf16)

    def xsend_d(k):
        for g in others_g:
            xd_copy(k, gr, g).start()
        for t in others_t:
            d_copy(k, gr, tp, t).start()

    def plane(k, w, g, i):
        c = col_of(g, i)

        @pl.when(c != fs)
        def _():
            p_copy(k, w, g, i).start()

        @pl.when(c == fs)
        def _():
            l_copy(k, w, g, i).start()

    def plane_own(k, w):
        for i in turn:
            plane(k, w, gr, i)

    def plane_x(k, w):
        for g in others_g:
            for i in turn:
                x_copy(k, w, i, g, gr).wait_recv()
                plane(k, w, g, i)

    def source(s):
        e = s // wing
        return lax.rem((fs // wing + e) * wing + lax.rem(fs + s, wing), n)

    def arrive(k, w):
        def forward(f):
            for t in others_t:
                f_copy(k, w, f, t).start()
            if hs[k]:
                v_copy(k, w, f, gr).start()

        @pl.when(is_recv)
        def _():
            l_copy(k, w, 0, 0).wait()
            forward(fs)

            def take(s):
                f = source(s)
                f_copy(k, w, f, tp).wait_recv()
                forward(f)
            loop(1, n, take)

    def cross(k, w):
        if hs[k]:
            @pl.when(is_recv)
            def _():
                def take(s):
                    f = source(s)
                    v_copy(k, w, f, 1 - gr).wait_recv()
                    for t in others_t:
                        fv_copy(k, w, f, t).start()
                loop(0, n, take)

    def landed(k, w):
        @pl.when(jnp.logical_not(is_recv))
        def _():
            def take(f):
                f_copy(k, w, f, tp).wait_recv()
                if hs[k]:
                    fv_copy(k, w, f, tp).wait_recv()
            loop(0, n, take)

    def relay_d(k):
        for g in others_g:
            xd_copy(k, g, gr).wait_recv()
            for t in others_t:
                d_copy(k, g, tp, t).start()

    def landed_d(k):
        for g in range(G):
            for t in others_t:
                d_copy(k, g, t, tp).wait_recv()

    def gather_done(k):
        for w in range(2):
            for i in range(q):
                for g in others_g:
                    x_copy(k, w, i, gr, g).wait_send()
            for g in range(G):
                for i in range(q):
                    @pl.when(col_of(g, i) != fs)
                    def _():
                        p_copy(k, w, g, i).wait_send()

            @pl.when(is_recv)
            def _():
                def sent(f):
                    for t in others_t:
                        f_copy(k, w, f, t).wait_send()
                        if hs[k]:
                            fv_copy(k, w, f, t).wait_send()
                    if hs[k]:
                        v_copy(k, w, f, gr).wait_send()
                loop(0, n, sent)
        for g in others_g:
            xd_copy(k, gr, g).wait_send()
        for g in range(G):
            for t in others_t:
                d_copy(k, g, tp, t).wait_send()

    def tokens(k):
        return (p if k == 0 else ag)[0].reshape(rows, D)

    def normed_of(x):
        return (x * lax.rsqrt(jnp.mean(x * x, axis=-1, keepdims=True) + norm_eps)).astype(bf16)

    def gates(k):
        ft = min(FFb, 256)

        def act(j):
            cols = pl.ds(j * ft, ft)
            gact[:, cols] = jnp.dot(tokens(k), wall[k, 0, :, :, cols].reshape(D, ft), preferred_element_type=f32)
        for j in range(FFb // ft):
            act(j)

    def compute(k):
        ft = min(FFb, 256)

        def act(j):
            cols = pl.ds(j * ft, ft)
            gate = gact[:, cols]
            up = jnp.dot(tokens(k), wall[k, 1, :, :, cols].reshape(D, ft), preferred_element_type=f32)
            hid[:, cols] = (gate / (1.0 + jnp.exp(-gate)) * up).astype(bf16)
        for j in range(FFb // ft):
            act(j)

        def proj(s):
            cols = pl.ds(s * DC, DC)
            v = jnp.dot(hid[...], dn[k, s], preferred_element_type=f32)
            p[k, :, :, cols] = v.reshape(n, tb, DC).astype(bf16)
        for s in range(G * T):
            proj(s)

    half = na // 2 if na % 2 == 0 else na
    far = na // half - 1
    pos = lax.rem(a, half)
    mirror = lax.rem(a + half, na)

    def near(d):
        return a - pos + lax.rem(pos + d, half)

    def across(a2):
        return lax.rem(a2 + half, na)

    def part(c):
        return pl.ds(c * tc, tc)

    def s1_copy(k, a2, c):
        return rc(p.at[k, 2 * a2 + 1 - b, part(c)], r1.at[k, a2, part(c)],
                  s1_s.at[k, a2, c], s1_r.at[k, a2, c], dev(gr, peer, tp))

    def s2_copy(k, a2, a_from, c):
        return rc(q2.at[k, a2, part(c)], r2.at[k, a_from, part(c)],
                  s2_s.at[k, a2, c], s2_r.at[k, a_from, c], dev(gr, 2 * a2 + b, tp))

    def s3_copy(k, o, a_from, c):
        return rc(q2.at[k, across(o), part(c)], r3.at[k, a_from, part(c)],
                  s3_s.at[k, o, c], s3_r.at[k, a_from, c], dev(gr, 2 * o + b, tp))

    def rs_first(k):
        def send(of):
            def chunks(d):
                for c in range(C):
                    s1_copy(k, of(d), c).start()
            return chunks
        if far:
            loop(1, half, send(lambda d: across(near(d))))
            send(lambda d: mirror)(0)
        loop(1, half, send(near))
        send(lambda d: a)(0)

    def pair(k, a2, c):
        s1_copy(k, a2, c).wait_recv()
        return p[k, 2 * a2 + b, part(c)].astype(f32) + r1[k, a2, part(c)].astype(f32)

    def rs_far(k, c):
        if far:
            def send(d):
                o = near(d)
                q2[k, across(o), part(c)] = pair(k, across(o), c).astype(bf16)
                s3_copy(k, o, a, c).start()
            loop(1, half, send)

    def rs_near(k, c):
        def send(d):
            o = near(d)
            q2[k, o, part(c)] = pair(k, o, c).astype(bf16)
            s2_copy(k, o, a, c).start()
        loop(1, half, send)

    def rs_mid(k, c):
        if far:
            sums[part(c)] = pair(k, mirror, c)

            def take(d):
                o = near(d)
                s3_copy(k, a, o, c).wait_recv()
                sums[part(c)] += r3[k, o, part(c)].astype(f32)
            loop(1, half, take)
            q2[k, mirror, part(c)] = sums[part(c)].astype(bf16)
            s2_copy(k, mirror, a, c).start()

    def rs_own(k, c):
        st[part(c)] += 0.5 * pair(k, a, c)

    def rs_last(k, c):
        def take(a2):
            s2_copy(k, a2, a2, c).wait_recv()
            st[part(c)] += 0.5 * r2[k, a2, part(c)].astype(f32)
        loop(1, half, lambda d: take(near(d)))
        if far:
            take(mirror)
        x = st[part(c)]
        ag[k, fs, part(c)] = normed_of(x) if k == 0 else x.astype(bf16)

        if far:
            z_copy(k, fs, mirror, c).start()

        def send(d):
            z_copy(k, fs, near(d), c).start()
        loop(1, half, send)
        y_copy(k, fs, c).start()

    def z_copy(k, j, a2, c):
        blk = ag.at[k, j, part(c)]
        return rc(blk, blk, g_s.at[k, a2, c], g_r.at[k, j, c], dev(gr, 2 * a2 + b, tp))

    def y_copy(k, j, c):
        blk = ag.at[k, j, part(c)]
        return rc(blk, blk, h_s.at[k, j // 2, c], g_r.at[k, j, c], dev(gr, peer, tp))

    def zz_copy(k, a2, c):
        blk = ag.at[k, 2 * mirror + b, part(c)]
        return rc(blk, blk, gg_s.at[k, a2, c], g_r.at[k, 2 * mirror + b, c], dev(gr, 2 * a2 + b, tp))

    def pass_on(k, a2, c):
        z_copy(k, 2 * a2 + b, a2, c).wait_recv()
        y_copy(k, 2 * a2 + b, c).start()

    def ag_pass(k, c):
        def own(d):
            pass_on(k, near(d), c)
        loop(1, half, own)
        if far:
            z_copy(k, 2 * mirror + b, a, c).wait_recv()

            def spread(d):
                zz_copy(k, near(d), c).start()
            loop(1, half, spread)
            y_copy(k, 2 * mirror + b, c).start()

    def ag_far(k, c):
        if far:
            def theirs(d):
                pass_on(k, across(near(d)), c)
            loop(1, half, theirs)

    def ag_take(k):
        for c in range(C):
            def take(a2):
                y_copy(k, 2 * a2 + 1 - b, c).wait_recv()
            loop(0, na, take)

    def rs_done(k):
        for c in range(C):
            def sent(a2):
                s1_copy(k, a2, c).wait_send()
            loop(0, na, sent)

            def sent2(d):
                s2_copy(k, near(d), a, c).wait_send()
                if far:
                    s3_copy(k, near(d), a, c).wait_send()
            loop(1, half, sent2)
            if far:
                s2_copy(k, mirror, a, c).wait_send()

    def ag_done(k):
        for c in range(C):
            def sent(d):
                z_copy(k, fs, near(d), c).wait_send()
                if far:
                    zz_copy(k, near(d), c).wait_send()
            loop(1, half, sent)
            if far:
                z_copy(k, fs, mirror, c).wait_send()

            def sent2(a2):
                y_copy(k, 2 * a2 + b, c).wait_send()
            loop(0, na, sent2)

    for load in loads:
        load.start()
    barrier = pltpu.get_barrier_semaphore()

    def greet(s):
        pl.semaphore_signal(barrier, inc=1, device_id=dev(gr, lax.rem(fs + s, n), tp), device_id_type=MESH)
    loop(1, n, greet)
    for t in others_t:
        pl.semaphore_signal(barrier, inc=1, device_id=dev(gr, fs, t), device_id_type=MESH)
    for g in others_g:
        pl.semaphore_signal(barrier, inc=1, device_id=dev(g, fs, tp), device_id_type=MESH)
    loads[0].wait()
    cast_w(0, 0)
    pl.semaphore_wait(barrier, n + T + G - 3)

    def norm_rows(j):
        p[0, j] = normed_of(prompt[j].astype(f32))

    def start_tokens():
        loads[7].wait()
        loop(0, n, norm_rows)
        st[...] = prompt[fs].astype(f32)

    def done(k):
        gather_done(k)
        rs_done(k)
        ag_done(k)

    xsend_w(0, 0)
    plane_own(0, 0)
    cast_w(0, 1)
    xsend_w(0, 1)
    plane_own(0, 1)
    cast_d(0)
    xsend_d(0)
    cast_w(1, 0)
    cast_w(1, 1)
    cast_d(1)
    start_tokens()
    xsend_w(1, 0)
    plane_x(0, 0)
    plane_x(0, 1)
    arrive(0, 0)
    arrive(0, 1)
    relay_d(0)
    cross(0, 0)
    landed(0, 0)
    xsend_w(1, 1)
    plane_x(1, 0)
    plane_own(1, 0)
    gates(0)
    cross(0, 1)
    landed(0, 1)
    plane_own(1, 1)
    landed_d(0)
    compute(0)
    rs_first(0)
    plane_x(1, 1)
    xsend_d(1)
    rs_far(0, 0)
    if C > 1:
        rs_far(0, 1)
    arrive(1, 0)
    rs_mid(0, 0)
    if C > 1:
        rs_mid(0, 1)
    rs_near(0, 0)
    if C > 1:
        rs_near(0, 1)
    rs_own(0, 0)
    if C > 1:
        rs_last(0, 0)
        rs_own(0, 1)
    arrive(1, 1)
    rs_last(0, C - 1)
    relay_d(1)
    ag_pass(0, 0)
    if C > 1:
        ag_pass(0, 1)
    ag_far(0, 0)
    if C > 1:
        ag_far(0, 1)
    cross(1, 0)
    ag_take(0)
    landed(1, 0)
    gates(1)
    cross(1, 1)
    landed(1, 1)
    landed_d(1)
    compute(1)
    rs_first(1)
    done(0)
    rs_far(1, 0)
    if C > 1:
        rs_far(1, 1)
    rs_mid(1, 0)
    if C > 1:
        rs_mid(1, 1)
    rs_near(1, 0)
    if C > 1:
        rs_near(1, 1)
    rs_own(1, 0)
    if C > 1:
        rs_last(1, 0)
        rs_own(1, 1)
    rs_last(1, C - 1)
    ag_pass(1, 0)
    if C > 1:
        ag_pass(1, 1)
    ag_far(1, 0)
    if C > 1:
        ag_far(1, 1)
    gather_done(1)
    rs_done(1)
    ag_take(1)
    ag_done(1)


def write_out(wall, dn, ag, gate_o, up_o, down_o, mixed_o, o_s, d_s, m_s):
    L, S, _, DC = dn.shape
    copies = []
    for k in range(L):
        copies.append(pltpu.make_async_copy(wall.at[k, 0], gate_o.at[k], o_s.at[k, 0]))
        copies.append(pltpu.make_async_copy(wall.at[k, 1], up_o.at[k], o_s.at[k, 1]))
        for s in range(S):
            copies.append(pltpu.make_async_copy(
                dn.at[k, s], down_o.at[k, :, pl.ds(s * DC, DC)], d_s.at[k, s]))
    copies.append(pltpu.make_async_copy(ag.at[L - 1], mixed_o, m_s))
    for c in copies:
        c.start()
    for c in copies:
        c.wait()


def per_device(G, n, T, prompt, norm_gain, gate_weight, up_weight, down_weight):
    D = prompt.shape[2]
    rows = prompt.shape[0] * prompt.shape[1]
    L, R, C_ = gate_weight.shape
    FFb, DC = down_weight.shape[1:]
    q = C_ // FFb
    tb = rows // n
    na = n // 2
    C = max(1, min(2, tb // 8))
    dma = pltpu.SemaphoreType.DMA
    vmem = pl.BlockSpec(memory_space=pltpu.VMEM)
    anym = pl.BlockSpec(memory_space=pl.ANY)
    wall, dn, ag = pl.pallas_call(
        functools.partial(kernel, G, n, T),
        out_shape=(
            pltpu.VMEM((L, 2, n, R, FFb), bf16),
            pltpu.VMEM((L, G * T, FFb, DC), bf16),
            pltpu.VMEM((L, n, tb, D), bf16),
        ),
        in_specs=[pl.BlockSpec(memory_space=pltpu.HBM)] * 5,
        out_specs=(vmem,) * 3,
        scratch_shapes=[
            pltpu.VMEM((n, tb, D), bf16), pltpu.VMEM((L, R), f32),
            pltpu.VMEM((L, R, C_), f32), pltpu.VMEM((L, R, C_), f32), pltpu.VMEM((L, FFb, DC), f32),
            dma((8,)),
            pltpu.VMEM((L, 2, G, q, R, FFb), bf16),
            pltpu.VMEM((L, n, tb, D), bf16),
            pltpu.VMEM((L, na, tb, D), bf16),
            pltpu.VMEM((L, na, tb, D), bf16),
            pltpu.VMEM((L, na, tb, D), bf16),
            pltpu.VMEM((L, na, tb, D), bf16),
            pltpu.VMEM((tb, D), f32),
            pltpu.VMEM((rows, FFb), bf16),
            pltpu.VMEM((rows, FFb), f32),
            pltpu.VMEM((tb, D), f32),
            dma((L, 2, q, G)), dma((L, 2, q, G)), dma((L, 2, n)), dma((L, 2, 2, n)), dma((L, G)),
            dma((L, 2, G, q)), dma((L, 2, n)), dma((L, 2)), dma((L, 2, 2, n, T)),
            dma((L, G, T)), dma((L, G * T)),
            dma((L, na, C)), dma((L, na, C)), dma((L, na, C)), dma((L, na, C)), dma((L, na, C)), dma((L, na, C)),
            dma((L, na, C)), dma((L, na, C)), dma((L, n, C)), dma((L, na, C)),
        ],
        compiler_params=pltpu.CompilerParams(
            collective_id=0, has_side_effects=True, vmem_limit_bytes=40 * 1024 * 1024),
    )(prompt.reshape(n, tb, D), norm_gain, gate_weight, up_weight, down_weight)
    gate, up, down, mixed = pl.pallas_call(
        write_out,
        out_shape=(
            jax.ShapeDtypeStruct((L, n, R, FFb), bf16),
            jax.ShapeDtypeStruct((L, n, R, FFb), bf16),
            jax.ShapeDtypeStruct((L, FFb, D), bf16),
            jax.ShapeDtypeStruct((n, tb, D), bf16),
        ),
        in_specs=[anym] * 3,
        out_specs=(anym,) * 4,
        scratch_shapes=[dma((L, 2)), dma((L, G * T)), dma(())],
        compiler_params=pltpu.CompilerParams(vmem_limit_bytes=1024 * 1024),
    )(*(pltpu.with_memory_space_constraint(x, pltpu.VMEM) for x in (wall, dn, ag)))
    return (gate.reshape(L, n * R, FFb), up.reshape(L, n * R, FFb), down, mixed.reshape(prompt.shape))


def solution(mesh):
    G, n, T = mesh.shape["gr"], mesh.shape["fs"], mesh.shape["tp"]
    in_specs = (
        P(("gr", "tp"), None, None),
        P(None, "fs"),
        P(None, "fs", ("gr", "tp")),
        P(None, "fs", ("gr", "tp")),
        P(None, "fs", ("gr", "tp")),
    )
    out_specs = (
        P(None, None, "fs"),
        P(None, None, "fs"),
        P(None, "fs", None),
        P(("gr", "tp"), None, None),
    )
    return jax.shard_map(
        functools.partial(per_device, G, n, T),
        mesh=mesh, in_specs=in_specs, out_specs=out_specs, check_vma=False)
```
